256 devices in a mesh: fs: 64 (over z, x, core), tp: 4 (over y).
Axes of the slice: x: 4, y: 4, z: 8, core: 2. Of those that a mesh axis runs over, the one named last changes fastest.
Arguments:
- inputs: bfloat16 [65536, 2048], P('fs'), may hold values from -16 to 16
- cotangents: bfloat16 [65536, 3, 1024], P('fs', None, 'tp'), may hold values from -0.0234375 to 0.0234375
- factors: bfloat16 [3, 2048, 256], P(None, 'fs'), may hold values from -13.810679 to 13.810679
- first_moment: float32 [3, 256, 1024], P(None, None, 'tp'), may hold values from -6 to 6
- second_moment: float32 [3, 256, 1024], P(None, None, 'tp'), may hold values from 0.05 to 1
- master: float32 [3, 2048, 1024], P(None, 'fs', 'tp'), may hold values from -0.125 to 0.125
Outputs:
- update_step: float32 [3, 2048, 1024], P(None, 'fs', 'tp')
- new_master: float32 [3, 2048, 1024], P(None, 'fs', 'tp')
- new_copy: bfloat16 [3, 2048, 1024], P(None, None, 'tp')
- new_first: float32 [3, 256, 1024], P(None, None, 'tp')
- new_second: float32 [3, 256, 1024], P(None, None, 'tp')
The draws below stay inside these ranges and needn't reach their ends.
All inputs are finite; a program needn't handle non-finite values.
Results may differ from the reference program's by a relative error of at most 0.001.
Values may be sent and summed in bfloat16 or wider, within the bound.
A program may use at most 64 MiB of HBM per device.

```python
import math
import jax
import jax.numpy as jnp
from jax import lax

D = 2048
MW = 1024
RANK = 256
MATS = 3
TOKENS = 65536


def draw_factors(key, part):
    keys = jax.random.split(jax.random.fold_in(key, 17), 3)
    position = jnp.arange(D, dtype=jnp.float32) / (D - 1)
    base = jnp.clip(jax.random.normal(keys[0], (MATS, D, RANK), jnp.float32), -5.0, 5.0)
    ramp = jnp.exp(math.log(5.0) * position)
    row_scale = jnp.exp(jax.random.uniform(keys[1], (MATS, D, 1), jnp.float32, 0.0, math.log(10.0)))
    col_scale = jnp.exp(jax.random.uniform(keys[2], (MATS, 1, RANK), jnp.float32, 0.0, math.log(10.0)))
    value = base * ramp[None, :, None] * row_scale * col_scale / (8.0 * math.sqrt(D))
    return value.astype(jnp.bfloat16)


def strengthened(values, stream_key, source, target, parts, factor):
    def block_of(axis_at):
        return (jnp.arange(values.shape[axis_at]) // (values.shape[axis_at] // parts)).reshape((-1,) + (1,) * (values.ndim - 1 - axis_at))

    one_side = jax.random.permutation(stream_key, parts)[block_of(target)]
    far = (block_of(target) + parts // 2) % parts
    return jnp.where((block_of(source) == one_side) | (block_of(source) == far), factor * values, values)


def block_levels(key, dims, pieces, least, high):
    factor_of = 1.0
    for dim, parts in pieces:
        heights = jax.random.uniform(jax.random.fold_in(jax.random.fold_in(key, 6), dim), (parts,), jnp.float32, least / len(pieces), high / len(pieces))
        factor_of = factor_of * jnp.repeat(jnp.exp(heights), dims[dim] // parts).reshape((-1,) + (1,) * (len(dims) - 1 - dim))
    return factor_of


def normal_values(rng, shape, deviation, bound, cuts=(), held_as=jnp.bfloat16):
    values = deviation * jax.random.normal(rng, shape, jnp.float32)
    if cuts:
        values = values * block_levels(rng, shape, cuts, -0.22, 0.18)
    return jnp.clip(values, -bound, bound).astype(held_as)


def noise_with(rng, shape, spread, limit, cuts, heavy, kind=jnp.bfloat16):
    entries = spread * jax.random.normal(rng, shape, jnp.float32)
    if cuts:
        entries = entries * block_levels(rng, shape, cuts, -0.22, 0.18)
    return jnp.clip(strengthened(entries, jax.random.fold_in(rng, 3), *heavy), -limit, limit).astype(kind)


def setup_inputs(seed: int = 0) -> dict:
    streams_of = jax.random.split(jax.random.key(seed), 7)
    inputs = noise_with(streams_of[0], (TOKENS, D), 1.0, 16.0, ((0, 64),), (0, 1, 64, 4.0))
    cotangents = normal_values(streams_of[1], (TOKENS, MATS, MW), (1.0 / TOKENS ** 0.5), 0.0234375, ((0, 64), (2, 4)))
    factors = draw_factors(jax.random.fold_in(streams_of[6], 71), 0)
    first_moment = normal_values(streams_of[3], (MATS, RANK, MW), 1.0, 6.0, ((2, 4),), jnp.float32)
    second_moment = jnp.clip(jnp.exp(math.log(1.0) - 2.9957323 * jax.random.uniform(streams_of[4], (MATS, RANK, MW), jnp.float32) ** block_levels(streams_of[4], (MATS, RANK, MW), ((2, 4),), -0.2, 0.2)), 0.05, 1.0)
    master = normal_values(streams_of[5], (MATS, D, MW), D ** -0.5, 0.125, ((1, 64), (2, 4)), jnp.float32)
    return {"inputs": inputs, "cotangents": cotangents, "factors": factors, "first_moment": first_moment, "second_moment": second_moment, "master": master}


beta_first = 0.8
beta_second = 0.9
adam_eps = 1e-08
norm_eps = 1e-06
learning_rate = 0.005

def reference(inputs, cotangents, factors, first_moment, second_moment, master):
    flat_cot = cotangents.reshape(cotangents.shape[0], MATS * MW)
    gradient = lax.dot_general(inputs, flat_cot, (((0,), (0,)), ((), ())), preferred_element_type=jnp.float32)
    gradient = gradient.reshape(D, MATS, MW).transpose(1, 0, 2)
    factor32 = factors.astype(jnp.float32)
    projected = jnp.einsum('mdr,mdc->mrc', factor32, gradient, precision=lax.Precision.HIGHEST)
    new_first = beta_first * first_moment + (1.0 - beta_first) * projected
    new_second = beta_second * second_moment + (1.0 - beta_second) * projected * projected
    normed = new_first / (jnp.sqrt(new_second) + adam_eps)
    update = jnp.einsum('mdr,mrc->mdc', factor32, normed, precision=lax.Precision.HIGHEST)
    root_mean = jnp.sqrt(lax.optimization_barrier(jnp.mean(update * update, axis=(1, 2))) + norm_eps)
    update_step = update / root_mean[:, None, None]
    new_master = master - learning_rate * update_step
    new_copy = new_master.astype(jnp.bfloat16)
    return (update_step, new_master, new_copy, new_first, new_second)
```

```python
import jax
import jax.numpy as jnp
from jax import lax
from jax.experimental import pallas as pl
from jax.experimental.pallas import tpu as pltpu
from jax.sharding import Mesh
from jax.sharding import PartitionSpec as P

D = 2048
MW = 1024
BF = jnp.bfloat16
F32 = jnp.float32
MESH = pl.DeviceIdType.MESH

beta_first = 0.8
beta_second = 0.9
adam_eps = 1e-08
norm_eps = 1e-06
learning_rate = 0.005

NZ, NX = 8, 4
GATHER_COPIES = 48


class Gather:
    def __init__(self, pos, first0, first1, ssem, rsem):
        self.z, self.x, self.c, self.y = pos
        self.b0, self.b1 = first0, first1
        self.ssem, self.rsem = ssem, rsem
        self.count = 0
        self.sent = []

    def at(self, dz=0, dx=0, other=False):
        z = lax.rem(self.z + (dz + NZ), NZ)
        x = lax.rem(self.x + (dx + NX), NX)
        return (z, x, 1 - self.c if other else self.c, self.y)

    def zof(self, dz):
        return lax.rem(self.z + (dz + NZ), NZ)

    def xof(self, dx):
        return lax.rem(self.x + (dx + NX), NX)

    def send(self, ref, target):
        k = self.count
        self.count += 1
        copy = pltpu.make_async_remote_copy(
            src_ref=ref, dst_ref=ref, send_sem=self.ssem.at[k], recv_sem=self.rsem.at[k], device_id=target, device_id_type=MESH
        )
        copy.start()
        self.sent.append(copy)
        return copy

    def pair(self, ref):
        self.pairs.append(self.send(ref, self.at(other=True)))

    def blk(self, dz, part=None):
        if part is None:
            return self.b0.at[self.c, self.zof(dz)]
        return self.b0.at[self.c, self.zof(dz), pl.ds(2 * part, 2)]

    def col(self, dx, part=None):
        if part is None:
            return self.b1.at[self.c, self.xof(dx)]
        return self.b1.at[self.c, self.xof(dx), pl.ds(4 * part, 4)]

    def stages(self):
        self.pairs = []
        c, z, x = self.c, self.z, self.x
        own0, own1 = self.b0.at[c, z, x], self.b1.at[c, x, z]
        near = [self.send(own0, self.at(dx=dx)) for dx in (1, -1, 2)]
        far = [self.send(own1, self.at(dz=dz)) for dz in (1, -1, 2, -2, 3, -3, 4)]
        yield
        for k in near:
            k.wait_recv()
        right = self.send(self.blk(0), self.at(dz=1))
        left = self.send(self.blk(0), self.at(dz=-1))
        self.pair(self.blk(0))
        yield
        for k in far:
            k.wait_recv()
        east = self.send(self.col(0), self.at(dx=1))
        west = self.send(self.col(0), self.at(dx=-1))
        self.pair(self.col(0))
        yield
        for step in (1, 2):
            right.wait_recv()
            left.wait_recv()
            right = self.send(self.blk(-step), self.at(dz=1))
            left = self.send(self.blk(step), self.at(dz=-1))
            self.pair(self.blk(-step))
            self.pair(self.blk(step))
            yield
            if step == 1:
                east.wait_recv()
                west.wait_recv()
                east = self.send(self.col(-1, 0), self.at(dx=1))
                west = self.send(self.col(1, 1), self.at(dx=-1))
                self.pair(self.col(-1))
                self.pair(self.col(1))
                yield
        right.wait_recv()
        left.wait_recv()
        right = self.send(self.blk(-3, 0), self.at(dz=1))
        left = self.send(self.blk(3, 1), self.at(dz=-1))
        self.pair(self.blk(-3))
        self.pair(self.blk(3))
        yield
        east.wait_recv()
        west.wait_recv()
        self.pair(self.col(2))
        yield
        right.wait_recv()
        left.wait_recv()
        self.pair(self.blk(4))
        yield
        for k in self.pairs:
            k.wait_recv()

    def drain(self):
        for k in self.sent:
            k.wait_send()


def split(value):
    high = value.astype(BF)
    return high, (value - high.astype(F32)).astype(BF)


def dot(a, b):
    return lax.dot_general(a, b, (((1,), (0,)), ((), ())), preferred_element_type=F32)


def dot_first(a, b):
    return lax.dot_general(a, b, (((0,), (0,)), ((), ())), preferred_element_type=F32)


def chunk_of(b0, b1, z, m):
    pieces = []
    for x in range(NX):
        for c in range(2):
            pieces.append(b0[c, z, x, m])
            pieces.append(b1[c, x, z, m])
    return jnp.concatenate(pieces, axis=0)


def kernel(
    inputs, cots, factors, first, second, master,
    out_step, out_master, out_copy, out_first, out_second,
    xin, cin, f0, f1, m0, m1, ghi, glo, fm, sm, um, own_f32, own_step, own_new, copy_v,
    pa, pb, ca, cb, sa, sb, rxa, rzb, ta, tb, rza, rxb, ga, gb, nhi, nlo, squares,
    lsem, osem, fs_sem, fr_sem, ms_sem, mr_sem, bs_sem, br_sem,
):
    z, x, c, y = (lax.axis_index(a) for a in ("z", "x", "c", "y"))
    pos = (z, x, c, y)

    local = []

    def load(src, dst):
        k = pltpu.make_async_copy(src, dst, lsem.at[len(local)])
        k.start()
        local.append(k)
        return k

    fl = [
        load(factors.at[:, pl.ds(0, 16), :], f0.at[c, z, x]),
        load(factors.at[:, pl.ds(16, 16), :], f1.at[c, x, z]),
    ]
    xl = load(inputs, xin)
    cl = load(cots, cin)
    ml = [
        load(master.at[:, pl.ds(0, 16), :], m0.at[c, z, x]),
        load(master.at[:, pl.ds(16, 16), :], m1.at[c, x, z]),
    ]
    el = [load(first, fm), load(second, sm), load(master, own_f32)]

    barrier = pltpu.get_barrier_semaphore()
    peers = []
    for dz in range(1, NZ):
        peers.append((lax.rem(z + dz, NZ), x, c, y))
    for dx in range(1, NX):
        peers.append((z, lax.rem(x + dx, NX), c, y))
    for dy in range(1, 4):
        peers.append((z, x, c, lax.rem(y + dy, 4)))
    peers.append((z, x, 1 - c, y))
    for peer in peers:
        pl.semaphore_signal(barrier, inc=1, device_id=peer, device_id_type=MESH)
    for k in fl:
        k.wait()
    pl.semaphore_wait(barrier, len(peers))

    def gradient(lo, hi):
        def body(zz, _):
            xs = xin[:, pl.ds(pl.multiple_of(zz * 256, 256), 256)]
            for m in range(3):
                g_hi, g_lo = split(dot_first(xs, cin[m]))
                ghi[m, zz] = g_hi
                glo[m, zz] = g_lo
            return 0
        lax.fori_loop(lo, hi, body, 0)

    fg = Gather(pos, f0, f1, fs_sem, fr_sem)
    fst = fg.stages()
    next(fst)
    xl.wait()
    cl.wait()
    gradient(0, 4)
    next(fst)
    gradient(4, 8)
    for _ in fst:
        pass

    mg = Gather(pos, m0, m1, ms_sem, mr_sem)
    mst = mg.stages()
    for k in ml:
        k.wait()
    next(mst)

    for m in range(3):
        def body(zz, acc):
            f = chunk_of(f0, f1, zz, m)
            return acc + dot_first(f, ghi[m, zz]) + dot_first(f, glo[m, zz])
        acc = lax.fori_loop(0, NZ, body, jnp.zeros((256, 256), F32))
        for half in range(2):
            part = acc[:, half * 128:(half + 1) * 128]
            if m < 2:
                for xx in range(NX):
                    pa[half, xx, m] = part[xx * 64:(xx + 1) * 64]
            else:
                for zz in range(NZ):
                    pb[half, zz] = part[zz * 32:(zz + 1) * 32]

    started = []

    def send(src, dst, target):
        k = len(started)
        copy = pltpu.make_async_remote_copy(
            src_ref=src, dst_ref=dst, send_sem=bs_sem.at[k], recv_sem=br_sem.at[k], device_id=target, device_id_type=MESH
        )
        copy.start()
        started.append(copy)
        return copy

    def got(copies):
        for k in copies:
            k.wait_recv()

    partner = (z, x, 1 - c, y)

    def zpeer(dz):
        return lax.rem(z + (dz + NZ), NZ)

    def xpeer(dx):
        return lax.rem(x + (dx + NX), NX)

    zorder = (4, 3, -3, 2, -2, 1, -1)
    xorder = (2, 1, -1)

    k1 = send(pb.at[1 - c], cb, partner)
    k2 = send(pa.at[1 - c], ca, partner)
    got([k1])
    sb[...] = pb[c] + cb[...]
    b1 = [send(sb.at[zpeer(dz)], rzb.at[i], (zpeer(dz), x, c, y)) for i, dz in enumerate(zorder)]
    got([k2])
    sa[...] = pa[c] + ca[...]
    a1 = [send(sa.at[xpeer(dx)], rxa.at[i], (z, xpeer(dx), c, y)) for i, dx in enumerate(xorder)]
    next(mst)
    got(a1)
    for m in range(2):
        tot = sa[x, m]
        for i in range(3):
            tot = tot + rxa[i, m]
        for zz in range(NZ):
            ta[zz, m] = tot[zz * 8:(zz + 1) * 8]
    a2 = [send(ta.at[zpeer(dz)], rza.at[i], (zpeer(dz), x, c, y)) for i, dz in enumerate(zorder)]
    got(b1)
    tot = sb[z]
    for i in range(7):
        tot = tot + rzb[i]
    for xx in range(NX):
        tb[xx] = tot[xx * 8:(xx + 1) * 8]
    b2 = [send(tb.at[xpeer(dx)], rxb.at[i], (z, xpeer(dx), c, y)) for i, dx in enumerate(xorder)]
    next(mst)
    got(b2)
    tot = tb[x]
    for i in range(3):
        tot = tot + rxb[i]
    gb[c, z, x] = tot
    b3 = [send(gb.at[c, z, x], gb.at[c, z, x], (z, xpeer(dx), c, y)) for dx in xorder]
    got(a2)
    tot = ta[z]
    for i in range(7):
        tot = tot + rza[i]
    ga[c, x, z] = tot
    a3 = [send(ga.at[c, x, z], ga.at[c, x, z], (zpeer(dz), x, c, y)) for dz in zorder]
    got(b3)
    b4 = [send(gb.at[c, z], gb.at[c, z], (zpeer(dz), x, c, y)) for dz in zorder]
    next(mst)
    got(a3)
    a4 = [send(ga.at[c, x], ga.at[c, x], (z, xpeer(dx), c, y)) for dx in xorder]
    next(mst)
    got(a4)
    ka = send(ga.at[c], ga.at[c], partner)
    got(b4)
    kb = send(gb.at[c], gb.at[c], partner)
    next(mst)
    got([ka, kb])

    for k in el:
        k.wait()
    outs = []

    def store(src, dst):
        k = pltpu.make_async_copy(src, dst, osem.at[len(outs)])
        k.start()
        outs.append(k)

    for m in range(3):
        for half in range(2):
            cols = slice(half * 128, (half + 1) * 128)
            if m < 2:
                proj = jnp.concatenate([ga[half, xx, zz, m] for xx in range(NX) for zz in range(NZ)], axis=0)
            else:
                proj = jnp.concatenate([gb[half, zz, xx] for zz in range(NZ) for xx in range(NX)], axis=0)
            nf = beta_first * fm[m, :, cols] + (1.0 - beta_first) * proj
            ns = beta_second * sm[m, :, cols] + (1.0 - beta_second) * proj * proj
            fm[m, :, cols] = nf
            sm[m, :, cols] = ns
            hi, lo = split(nf / (jnp.sqrt(ns) + adam_eps))
            nhi[m, :, cols] = hi
            nlo[m, :, cols] = lo
    store(fm, out_first)
    store(sm, out_second)
    next(mst)
    ys = []
    for m in range(3):
        def body(zz, acc):
            f = chunk_of(f0, f1, zz, m)
            u = dot(f, nhi[m]) + dot(f, nlo[m])
            um[m, pl.ds(pl.multiple_of(zz * 256, 256), 256), :] = u
            uu = (u * u).reshape(32, 8, 256)
            uu = jnp.sum(uu, axis=0)
            return acc + uu[:, :128] + uu[:, 128:]
        squares[y, m] = lax.fori_loop(0, NZ, body, jnp.zeros((8, 128), F32))
        ys += [send(squares.at[y, m], squares.at[y, m], (z, x, c, lax.rem(y + dy, 4))) for dy in (1, 2, 3)]
        if m < 2:
            next(mst)
    for _ in mst:
        pass
    got(ys)

    rows = pl.multiple_of(z * 256 + x * 64 + c * 32, 32)
    for m in range(3):
        tot = squares[0, m]
        for j in range(1, 4):
            tot = tot + squares[j, m]
        inv = 1.0 / jnp.sqrt(jnp.sum(tot, keepdims=True) / (D * MW) + norm_eps)
        step = um[m, pl.ds(rows, 32), :] * inv
        own_step[m] = step
        own_new[m] = own_f32[m] - learning_rate * step

        def body(zz, _):
            at = pl.ds(pl.multiple_of(zz * 256, 256), 256)
            copy_v[m, at, :] = (chunk_of(m0, m1, zz, m) - learning_rate * (um[m, at, :] * inv)).astype(BF)
            return 0
        lax.fori_loop(0, NZ, body, 0)
        store(copy_v.at[m], out_copy.at[m])
    store(own_step, out_step)
    store(own_new, out_master)
    fg.drain()
    mg.drain()
    for k in started:
        k.wait_send()
    for k in outs:
        k.wait()


def local(inputs, cotangents, factors, first_moment, second_moment, master):
    cots = jnp.transpose(cotangents, (1, 0, 2))
    anyspace = pl.BlockSpec(memory_space=pl.ANY)
    V = pltpu.VMEM
    dma = pltpu.SemaphoreType.DMA
    return pl.pallas_call(
        kernel,
        out_shape=(
            jax.ShapeDtypeStruct((3, 32, 256), F32),
            jax.ShapeDtypeStruct((3, 32, 256), F32),
            jax.ShapeDtypeStruct((3, D, 256), BF),
            jax.ShapeDtypeStruct((3, 256, 256), F32),
            jax.ShapeDtypeStruct((3, 256, 256), F32),
        ),
        in_specs=[anyspace] * 6,
        out_specs=(anyspace,) * 5,
        scratch_shapes=[
            V((1024, 2048), BF), V((3, 1024, 256), BF),
            V((2, NZ, NX, 3, 16, 256), BF), V((2, NX, NZ, 3, 16, 256), BF),
            V((2, NZ, NX, 3, 16, 256), F32), V((2, NX, NZ, 3, 16, 256), F32),
            V((3, NZ, 256, 256), BF), V((3, NZ, 256, 256), BF),
            V((3, 256, 256), F32), V((3, 256, 256), F32), V((3, D, 256), F32),
            V((3, 32, 256), F32), V((3, 32, 256), F32), V((3, 32, 256), F32), V((3, D, 256), BF),
            V((2, NX, 2, 64, 128), F32), V((2, NZ, 32, 128), F32),
            V((NX, 2, 64, 128), F32), V((NZ, 32, 128), F32),
            V((NX, 2, 64, 128), F32), V((NZ, 32, 128), F32),
            V((3, 2, 64, 128), F32), V((7, 32, 128), F32),
            V((NZ, 2, 8, 128), F32), V((NX, 8, 128), F32),
            V((7, 2, 8, 128), F32), V((3, 8, 128), F32),
            V((2, NX, NZ, 2, 8, 128), F32), V((2, NZ, NX, 8, 128), F32),
            V((3, 256, 256), BF), V((3, 256, 256), BF), V((4, 3, 8, 128), F32),
            dma((16,)), dma((8,)),
            dma((GATHER_COPIES,)), dma((GATHER_COPIES,)), dma((GATHER_COPIES,)), dma((GATHER_COPIES,)),
            dma((64,)), dma((64,)),
        ],
        compiler_params=pltpu.CompilerParams(collective_id=0, has_side_effects=True, vmem_limit_bytes=60 * 1024 * 1024),
        name="update",
    )(inputs, cots, factors, first_moment, second_moment, master)


def solution(mesh):
    torus = Mesh(mesh.devices.reshape(NZ, NX, 2, mesh.shape["tp"]), ("z", "x", "c", "y"))
    fs = ("z", "x", "c")
    return jax.shard_map(
        local,
        mesh=torus,
        in_specs=(
            P(fs, None),
            P(fs, None, "y"),
            P(None, fs, None),
            P(None, None, "y"),
            P(None, None, "y"),
            P(None, fs, "y"),
        ),
        out_specs=(
            P(None, fs, "y"),
            P(None, fs, "y"),
            P(None, None, "y"),
            P(None, None, "y"),
            P(None, None, "y"),
        ),
        check_vma=False,
    )
```

```python
import jax
import jax.numpy as jnp
from jax import lax
from jax.experimental import pallas as pl
from jax.experimental.pallas import tpu as pltpu
from jax.sharding import Mesh
from jax.sharding import PartitionSpec as P

D = 2048
MW = 1024
BF = jnp.bfloat16
F32 = jnp.float32
MESH = pl.DeviceIdType.MESH

beta_first = 0.8
beta_second = 0.9
adam_eps = 1e-08
norm_eps = 1e-06
learning_rate = 0.005

NZ, NX = 8, 4
GATHER_COPIES = 96
ORDER = (2, 0, 1)


class Gather:
    def __init__(self, pos, whole, ssem, rsem, flip):
        self.z, self.x, self.c, self.y = pos
        self.b = whole
        self.ssem, self.rsem = ssem, rsem
        self.flip = flip
        self.sent = []
        self.waiting = {}
        self.pairs = {m: [] for m in range(3)}
        self.rest = []

    def zof(self, dz):
        return lax.rem(self.z + (dz + NZ), NZ)

    def xof(self, dx):
        return lax.rem(self.x + (dx + NX), NX)

    def send(self, ref, dz=0, dx=0, other=False, key=None):
        k = len(self.sent)
        copy = pltpu.make_async_remote_copy(
            src_ref=ref, dst_ref=ref, send_sem=self.ssem.at[k], recv_sem=self.rsem.at[k],
            device_id=(self.zof(dz), self.xof(dx), 1 - self.c if other else self.c, self.y), device_id_type=MESH,
        )
        copy.start()
        self.sent.append(copy)
        if key is not None:
            self.waiting[key] = copy
        return copy

    def got(self, key):
        self.waiting.pop(key).wait_recv()

    def blk(self, dz, m, part=None):
        xs = slice(None) if part is None else pl.ds(2 * part, 2)
        return self.b.at[m, self.zof(dz), xs, self.c, 0]

    def one(self, dz, dx):
        return self.b.at[:, self.zof(dz), self.xof(dx), self.c, 1]

    def start(self):
        own = self.b.at[:, self.z, self.x, self.c, 0]
        for dx in (2, 1, -1):
            self.send(own, dx=dx, key=("near", dx))
        own = self.one(0, 0)
        self.send(own, dz=1, key=("far", 1, -1))
        self.send(own, dz=-1, key=("far", 1, 1))
        self.cross_start(0)

    def cross_start(self, dz):
        self.send(self.one(dz, 0), dx=1, key=("cross", dz, -1))
        self.send(self.one(dz, 0), dx=-1, key=("cross", dz, 1))

    def near(self):
        for dx in (2, 1, -1):
            self.got(("near", dx))
        for m in ORDER:
            self.send(self.blk(0, m), dz=1, key=("ring", 1, m, -1))
            self.send(self.blk(0, m), dz=-1, key=("ring", 1, m, 1))
        for m in ORDER:
            self.pairs[m].append(self.send(self.blk(0, m), other=True))

    def ring(self, k, m):
        for side in (-1, 1):
            self.got(("ring", k, m, side))
            if k < 4:
                part = None if k < 3 else (0 if side < 0 else 1)
                self.send(self.blk(side * k, m, part), dz=-side, key=("ring", k + 1, m, side))
        if k < 4:
            for side in (-1, 1):
                self.pairs[m].append(self.send(self.blk(side * k, m), other=True))
        else:
            self.pairs[m].append(self.send(self.blk(4, m), other=True))

    def far(self, k):
        for side in (-1, 1) if k < 4 else (self.flip,):
            self.got(("far", k, side))
            if k < 3 or (k == 3 and side == self.flip):
                self.send(self.one(side * k, 0), dz=-side, key=("far", k + 1, side))
            self.cross_start(side * k)

    def cross(self, k):
        for dz in ((k, -k) if 0 < k < 4 else (self.flip * k,)):
            side = self.flip if dz % 2 else -self.flip
            for dx in (-1, 1):
                self.got(("cross", dz, dx))
            self.send(self.one(dz, side), dx=-side, key=("cross2", dz))

    def cross2(self, k):
        for dz in ((k, -k) if 0 < k < 4 else (self.flip * k,)):
            self.got(("cross2", dz))
            self.rest.append(self.send(self.b.at[:, self.zof(dz), :, self.c, 1], other=True))

    def paired(self, m):
        for k in self.pairs[m] + self.rest:
            k.wait_recv()
        self.rest = []

    def drain(self):
        for k in self.sent:
            k.wait_send()


def split(value):
    high = value.astype(BF)
    return high, (value - high.astype(F32)).astype(BF)


FLOOR = 2.0 ** -124


def coded(value):
    t = jnp.abs(value) * 8.0
    t = t * t
    t = t * t
    t = t * t * 2.0 ** 60
    t = jnp.maximum(t * t, FLOOR)
    return jnp.where(value < 0, -t, t).astype(BF)


def decoded(code):
    t = code.astype(F32)
    size = jnp.abs(t)
    root = lax.rsqrt(lax.rsqrt(lax.rsqrt(lax.rsqrt(size)))) * (2.0 ** -7.5 / 8.0)
    root = jnp.where(size > FLOOR, root, 0.0)
    return jnp.where(t < 0, -root, root)


def dot(a, b):
    return lax.dot_general(a, b, (((1,), (0,)), ((), ())), preferred_element_type=F32)


def kernel(
    inputs, cots, factors, first, second, master,
    own_step, own_new, copy_v, fm, sm,
    xin, cin, ct, fw, mw, wide, gt, um, own_f32,
    pa, pb, ca, cb, sa, sb, rxa, rzb, ta, tb, rza, rxb, ga, gb, nn, squares,
    lsem, fs_sem, fr_sem, ms_sem, mr_sem, bs_sem, br_sem,
):
    z, x, c, y = (lax.axis_index(a) for a in ("z", "x", "c", "y"))
    pos = (z, x, c, y)

    local = []

    def load(src, dst):
        k = pltpu.make_async_copy(src, dst, lsem.at[len(local)])
        k.start()
        local.append(k)
        return k

    fl = [
        load(factors.at[:, pl.ds(16 * h, 16), :], fw.at[:, z, x, c, h]) for h in range(2)
    ]
    ml = load(master, own_f32)
    cl = load(cots, cin)
    xl = load(inputs, xin)
    el = [load(first, fm), load(second, sm)]

    barrier = pltpu.get_barrier_semaphore()
    peers = []
    for dz in range(1, NZ):
        peers.append((lax.rem(z + dz, NZ), x, c, y))
    for dx in range(1, NX):
        peers.append((z, lax.rem(x + dx, NX), c, y))
    for dy in range(1, 4):
        peers.append((z, x, c, lax.rem(y + dy, 4)))
    peers.append((z, x, 1 - c, y))
    for peer in peers:
        pl.semaphore_signal(barrier, inc=1, device_id=peer, device_id_type=MESH)
    ml.wait()
    for m in range(3):
        for h in range(2):
            mw[m, z, x, c, h] = coded(own_f32[m, 16 * h:16 * h + 16, :])
    for k in fl:
        k.wait()
    pl.semaphore_wait(barrier, len(peers))

    def turned(m):
        ct[pl.ds(256 * m, 256), :] = cin[m].T

    def gradient(lo, hi):
        def body(zz, _):
            at = pl.ds(pl.multiple_of(zz * 256, 256), 256)
            g_hi, g_lo = split(dot(ct[...], xin[:, at]))
            for m in range(3):
                gt[m, 0:256, at] = g_hi[256 * m:256 * (m + 1)]
                gt[m, 256:512, at] = g_lo[256 * m:256 * (m + 1)]
            return 0
        lax.fori_loop(lo, hi, body, 0)

    f = Gather(pos, fw, fs_sem, fr_sem, -1)
    w = Gather(pos, mw, ms_sem, mr_sem, 1)
    f.start()
    w.start()
    cl.wait()
    for m in range(3):
        turned(m)
    xl.wait()
    gradient(0, 3)
    f.near()
    f.far(1)
    f.cross(0)
    w.near()
    gradient(3, 5)
    for m in ORDER:
        f.ring(1, m)
    f.far(2)
    f.cross(1)
    f.cross2(0)
    w.far(1)
    w.cross(0)
    gradient(5, 7)
    for m in ORDER:
        f.ring(2, m)
    for m in ORDER:
        w.ring(1, m)
    f.far(3)
    f.cross(2)
    f.cross2(1)
    w.far(2)
    w.cross(1)
    w.cross2(0)
    gradient(7, 8)
    for m in ORDER:
        f.ring(3, m)
    f.far(4)
    f.cross(3)
    f.cross2(2)
    for m in ORDER:
        w.ring(2, m)
    f.cross(4)
    f.cross2(3)
    w.far(3)
    w.cross(2)
    w.cross2(1)
    f.cross2(4)
    f.ring(4, 2)
    f.ring(4, 0)
    f.ring(4, 1)

    started = []

    def send(src, dst, target):
        k = len(started)
        copy = pltpu.make_async_remote_copy(
            src_ref=src, dst_ref=dst, send_sem=bs_sem.at[k], recv_sem=br_sem.at[k], device_id=target, device_id_type=MESH
        )
        copy.start()
        started.append(copy)
        return copy

    def got(copies):
        for k in copies:
            k.wait_recv()

    partner = (z, x, 1 - c, y)

    def zpeer(dz):
        return lax.rem(z + (dz + NZ), NZ)

    def xpeer(dx):
        return lax.rem(x + (dx + NX), NX)

    zorder = (4, 3, -3, 2, -2, 1, -1)
    xorder = (2, 1, -1)

    def project(m):
        both = dot(gt[m], fw[m].reshape(D, 256))
        part = (both[:256] + both[256:]).T
        for half in range(2):
            cols = part[:, half * 128:(half + 1) * 128]
            if m < 2:
                for xx in range(NX):
                    pa[half, xx, m] = cols[xx * 64:(xx + 1) * 64]
            else:
                for zz in range(NZ):
                    pb[half, zz] = cols[zz * 32:(zz + 1) * 32]

    f.paired(2)
    project(2)
    k1 = send(pb.at[1 - c], cb, partner)
    f.paired(0)
    project(0)
    f.paired(1)
    project(1)
    k2 = send(pa.at[1 - c], ca, partner)
    for m in ORDER:
        w.ring(3, m)
    got([k1])
    sb[...] = pb[c] + cb[...]
    b1 = [send(sb.at[zpeer(dz)], rzb.at[i], (zpeer(dz), x, c, y)) for i, dz in enumerate(zorder)]
    got([k2])
    sa[...] = pa[c] + ca[...]
    a1 = [send(sa.at[xpeer(dx)], rxa.at[i], (z, xpeer(dx), c, y)) for i, dx in enumerate(xorder)]
    w.far(4)
    w.cross(3)
    w.cross2(2)
    got(a1)
    for m in range(2):
        tot = sa[x, m]
        for i in range(3):
            tot = tot + rxa[i, m]
        for zz in range(NZ):
            ta[zz, m] = tot[zz * 8:(zz + 1) * 8]
    a2 = [send(ta.at[zpeer(dz)], rza.at[i], (zpeer(dz), x, c, y)) for i, dz in enumerate(zorder)]
    w.cross(4)
    w.cross2(3)
    got(b1)
    tot = sb[z]
    for i in range(7):
        tot = tot + rzb[i]
    for xx in range(NX):
        tb[xx] = tot[xx * 8:(xx + 1) * 8]
    b2 = [send(tb.at[xpeer(dx)], rxb.at[i], (z, xpeer(dx), c, y)) for i, dx in enumerate(xorder)]
    w.cross2(4)
    for m in ORDER:
        w.ring(4, m)
    got(b2)
    tot = tb[x]
    for i in range(3):
        tot = tot + rxb[i]
    gb[c, z, x] = tot
    b3 = [send(gb.at[c, z, x], gb.at[c, z, x], (z, xpeer(dx), c, y)) for dx in xorder]
    got(a2)
    tot = ta[z]
    for i in range(7):
        tot = tot + rza[i]
    ga[c, x, z] = tot
    a3 = [send(ga.at[c, x, z], ga.at[c, x, z], (zpeer(dz), x, c, y)) for dz in zorder]

    def widen(m):
        def body(zz, _):
            wide[m, pl.ds(pl.multiple_of(zz * 256, 256), 256), :] = decoded(mw[m, zz].reshape(256, 256))
            return 0
        lax.fori_loop(0, NZ, body, 0)

    w.paired(2)
    widen(2)
    got(b3)
    b4 = [send(gb.at[c, z], gb.at[c, z], (zpeer(dz), x, c, y)) for dz in zorder]
    w.paired(0)
    widen(0)
    got(a3)
    a4 = [send(ga.at[c, x], ga.at[c, x], (z, xpeer(dx), c, y)) for dx in xorder]
    ka = [send(ga.at[c, x], ga.at[c, x], partner)]
    w.paired(1)
    widen(1)
    got(b4)
    kb = send(gb.at[c], gb.at[c], partner)
    for k in el:
        k.wait()
    got([kb])

    def moments(m):
        for half in range(2):
            cols = slice(half * 128, (half + 1) * 128)
            if m < 2:
                proj = jnp.concatenate([ga[half, xx, zz, m] for xx in range(NX) for zz in range(NZ)], axis=0)
            else:
                proj = jnp.concatenate([gb[half, zz, xx] for zz in range(NZ) for xx in range(NX)], axis=0)
            nf = beta_first * fm[m, :, cols] + (1.0 - beta_first) * proj
            ns = beta_second * sm[m, :, cols] + (1.0 - beta_second) * proj * proj
            fm[m, :, cols] = nf
            sm[m, :, cols] = ns
            hi, lo = split(nf / (jnp.sqrt(ns) + adam_eps))
            nn[m, 0:256, cols] = hi
            nn[m, 256:512, cols] = lo

    ys = {}

    def update(m):
        def body(zz, acc):
            fz = fw[m, pl.ds(2 * zz, 2)].reshape(512, 256)
            u = dot(jnp.concatenate([fz, fz], axis=1), nn[m])
            um[m, pl.ds(pl.multiple_of(zz * 512, 512), 512), :] = u
            uu = jnp.sum((u * u).reshape(64, 8, 256), axis=0)
            return acc + uu[:, :128] + uu[:, 128:]
        squares[y, m] = lax.fori_loop(0, 4, body, jnp.zeros((8, 128), F32))
        ys[m] = [send(squares.at[y, m], squares.at[y, m], (z, x, c, lax.rem(y + dy, 4))) for dy in (1, 2, 3)]

    moments(2)
    update(2)
    for i, dx in enumerate(xorder):
        got([a4[i]])
        ka.append(send(ga.at[c, xpeer(-dx)], ga.at[c, xpeer(-dx)], partner))
    got(ka)
    for m in (0, 1):
        moments(m)
        update(m)

    rows = pl.multiple_of(z * 256 + x * 64 + c * 32, 32)
    for m in ORDER:
        got(ys[m])
        tot = squares[0, m]
        for j in range(1, 4):
            tot = tot + squares[j, m]
        inv = 1.0 / jnp.sqrt(jnp.sum(tot, keepdims=True) / (D * MW) + norm_eps)
        step = um[m, pl.ds(rows, 32), :] * inv
        own_step[m] = step
        own_new[m] = own_f32[m] - learning_rate * step

        def body(zz, _):
            at = pl.ds(pl.multiple_of(zz * 256, 256), 256)
            copy_v[m, at, :] = (wide[m, at, :] - learning_rate * (um[m, at, :] * inv)).astype(BF)
            return 0
        lax.fori_loop(0, NZ, body, 0)
    f.drain()
    w.drain()
    for k in started:
        k.wait_send()


def write_out(*refs):
    sem = refs[-1]
    copies = [pltpu.make_async_copy(refs[i], refs[5 + i], sem.at[i]) for i in range(5)]
    for k in copies:
        k.start()
    for k in copies:
        k.wait()


def local(inputs, cotangents, factors, first_moment, second_moment, master):
    cots = jnp.transpose(cotangents, (1, 0, 2))
    hbm = pl.BlockSpec(memory_space=pltpu.HBM)
    V = pltpu.VMEM
    dma = pltpu.SemaphoreType.DMA
    results = pl.pallas_call(
        kernel,
        out_shape=(
            V((3, 32, 256), F32), V((3, 32, 256), F32), V((3, D, 256), BF), V((3, 256, 256), F32), V((3, 256, 256), F32),
        ),
        in_specs=[hbm] * 6,
        out_specs=(pl.BlockSpec(memory_space=pltpu.VMEM),) * 5,
        scratch_shapes=[
            V((1024, 2048), BF), V((3, 1024, 256), BF), V((768, 1024), BF),
            V((3, NZ, NX, 2, 2, 16, 256), BF), V((3, NZ, NX, 2, 2, 16, 256), BF), V((3, D, 256), F32),
            V((3, 512, D), BF), V((3, D, 256), F32), V((3, 32, 256), F32),
            V((2, NX, 2, 64, 128), F32), V((2, NZ, 32, 128), F32),
            V((NX, 2, 64, 128), F32), V((NZ, 32, 128), F32),
            V((NX, 2, 64, 128), F32), V((NZ, 32, 128), F32),
            V((3, 2, 64, 128), F32), V((7, 32, 128), F32),
            V((NZ, 2, 8, 128), F32), V((NX, 8, 128), F32),
            V((7, 2, 8, 128), F32), V((3, 8, 128), F32),
            V((2, NX, NZ, 2, 8, 128), F32), V((2, NZ, NX, 8, 128), F32),
            V((3, 512, 256), BF), V((4, 3, 8, 128), F32),
            dma((16,)),
            dma((GATHER_COPIES,)), dma((GATHER_COPIES,)), dma((GATHER_COPIES,)), dma((GATHER_COPIES,)),
            dma((64,)), dma((64,)),
        ],
        compiler_params=pltpu.CompilerParams(collective_id=0, has_side_effects=True, vmem_limit_bytes=58 * 1024 * 1024),
        name="update",
    )(inputs, cots, factors, first_moment, second_moment, master)
    return pl.pallas_call(
        write_out,
        out_shape=tuple(jax.ShapeDtypeStruct(r.shape, r.dtype) for r in results),
        in_specs=[pl.BlockSpec(memory_space=pl.ANY)] * 5,
        out_specs=(hbm,) * 5,
        scratch_shapes=[dma((5,))],
        compiler_params=pltpu.CompilerParams(vmem_limit_bytes=1024 * 1024),
        name="write_out",
    )(*results)


def solution(mesh):
    torus = Mesh(mesh.devices.reshape(NZ, NX, 2, mesh.shape["tp"]), ("z", "x", "c", "y"))
    fs = ("z", "x", "c")
    return jax.shard_map(
        local,
        mesh=torus,
        in_specs=(
            P(fs, None),
            P(fs, None, "y"),
            P(None, fs, None),
            P(None, None, "y"),
            P(None, None, "y"),
            P(None, fs, "y"),
        ),
        out_specs=(
            P(None, fs, "y"),
            P(None, fs, "y"),
            P(None, None, "y"),
            P(None, None, "y"),
            P(None, None, "y"),
        ),
        check_vma=False,
    )
```

```python
import math

import jax
import jax.numpy as jnp
from jax import lax
from jax.experimental import pallas as pl
from jax.experimental.pallas import tpu as pltpu
from jax.sharding import Mesh
from jax.sharding import PartitionSpec as P

D = 2048
MW = 1024
BF = jnp.bfloat16
F32 = jnp.float32
MESH = pl.DeviceIdType.MESH

beta_first = 0.8
beta_second = 0.9
adam_eps = 1e-08
norm_eps = 1e-06
learning_rate = 0.005

NZ, NX = 8, 4
GROUPS = 40
ORDER = (0, 1, 2)


class Copies:
    def __init__(self, pos, ssem, rsem, room):
        self.z, self.x, self.c, self.y = pos
        self.ssem, self.rsem, self.room = ssem, rsem, room
        self.sent = 0
        self.groups = {}

    def zof(self, dz):
        return lax.rem(self.z + (dz + NZ), NZ)

    def xof(self, dx):
        return lax.rem(self.x + (dx + NX), NX)

    def send(self, key, src, dst=None, dz=0, dx=0, dy=0, other=False):
        dst = src if dst is None else dst
        if key not in self.groups:
            self.groups[key] = [len(self.groups), 0]
        group = self.groups[key]
        size = math.prod(src.shape) * jnp.dtype(src.dtype).itemsize
        group[1] += size
        self.sent += size
        pltpu.make_async_remote_copy(
            src_ref=src, dst_ref=dst, send_sem=self.ssem.at[0], recv_sem=self.rsem.at[group[0]],
            device_id=(self.zof(dz), self.xof(dx), 1 - self.c if other else self.c, lax.rem(self.y + dy, 4)), device_id_type=MESH,
        ).start()

    def bytes_at(self, sem, size):
        part = self.room.at[pl.ds(0, size // 4096)]
        pltpu.make_async_copy(part, part, sem).wait()

    def got(self, key):
        self.bytes_at(self.rsem.at[self.groups[key][0]], self.groups[key][1])

    def drain(self):
        self.bytes_at(self.ssem.at[0], self.sent)


class Gather(Copies):
    def __init__(self, pos, whole, ssem, rsem, room, flip, rows):
        super().__init__(pos, ssem, rsem, room)
        self.b = whole
        self.flip = flip
        self.q0, self.q1 = pl.ds(0, rows // 8), pl.ds(rows // 8, 4 - rows // 8)

    def blk(self, dz, m, part=None):
        xs = slice(None) if part is None else pl.ds(2 * part, 2)
        return self.b.at[m, self.zof(dz), xs, self.c, self.q0]

    def one(self, dz, dx):
        return self.b.at[:, self.zof(dz), self.xof(dx), self.c, self.q1]

    def line(self, dz):
        return self.b.at[:, self.zof(dz), :, self.c, self.q1]

    def start_x(self):
        own = self.b.at[:, self.z, self.x, self.c, self.q0]
        for dx in (2, 1, -1):
            self.send("near", own, dx=dx)

    def cross_start(self, k, offsets):
        for dz in offsets:
            for dx in (1, -1):
                self.send(("cross", k), self.one(dz, 0), dx=dx)

    def cross_on(self, k, offsets):
        self.got(("cross", k))
        for dz in offsets:
            side = self.flip if dz % 2 else -self.flip
            self.send(("cross2", k), self.one(dz, side), dx=-side)

    def cross_end(self, k, offsets, key):
        self.got(("cross2", k))
        for dz in offsets:
            self.send(key, self.line(dz), other=True)


NEAR_Z, FAR_Z = (1, -1, 2, -2), (3, -3, 4)


class Direct(Gather):
    def own0(self):
        return self.b.at[pl.ds(0, 2), self.z, :, self.c, self.q0]

    def one(self, dz, dx):
        return self.b.at[pl.ds(0, 2), self.zof(dz), self.xof(dx), self.c, self.q1]

    def line(self, dz):
        return self.b.at[pl.ds(0, 2), self.zof(dz), :, self.c, self.q1]

    def column(self, dx):
        return self.b.at[2, :, self.xof(dx), self.c, self.y]

    def start(self):
        own = self.b.at[pl.ds(0, 2), self.z, self.x, self.c, self.q0]
        for dx in (2, 1, -1):
            self.send("near", own, dx=dx)
        own = self.b.at[2, self.z, self.x, self.c, self.y]
        for dz in FAR_Z + NEAR_Z:
            self.send("quarter", own, dz=dz)
        for dz in NEAR_Z:
            self.send(("far", 1), self.one(0, 0), dz=dz)
        self.line_start(0, (0,))
        for dz in FAR_Z:
            self.send(("far", 2), self.one(0, 0), dz=dz)

    def line_start(self, k, offsets):
        for dz in offsets:
            for dx in (2, 1, -1):
                self.send(("cross", k), self.one(dz, 0), dx=dx)

    def near(self):
        self.got("near")
        for k, offsets in ((1, NEAR_Z), (2, FAR_Z)):
            for dz in offsets:
                self.send(("ring", k), self.own0(), dz=dz)
        self.send("early", self.own0(), other=True)

    def quarter(self):
        self.got("quarter")
        for dx in (2, 1, -1):
            self.send("columns", self.column(0), dx=dx)
        for dy in (2, 1, 3):
            self.send("exchange", self.column(0), dy=dy)

    def columns(self):
        self.got("columns")
        for dx in (1, -1, 2):
            for dy in (2, 1, 3):
                self.send("exchange", self.column(dx), dy=dy)
        self.send("last", self.b.at[2, :, :, self.c, self.y], other=True)

    def exchange(self):
        self.got("exchange")
        for dy in (1, 2, 3):
            self.send("last", self.b.at[2, :, :, self.c, lax.rem(self.y + dy, 4)], other=True)

    def ring(self, k, offsets, key):
        self.got(("ring", k))
        for dz in offsets:
            self.send(key, self.b.at[pl.ds(0, 2), self.zof(dz), :, self.c, self.q0], other=True)

    def far(self, k, offsets):
        self.got(("far", k))
        self.line_start(k, offsets)

    def line_end(self, k, offsets, key):
        self.got(("cross", k))
        for dz in offsets:
            self.send(key, self.line(dz), other=True)


class Ring(Gather):
    def both(self, k):
        return (k, -k) if 0 < k < 4 else (self.flip * k,)

    def start(self):
        self.start_x()
        for dz in (1, -1):
            self.send(("far", 1), self.one(0, 0), dz=dz)
        self.cross_start(0, (0,))

    def near(self):
        self.got("near")
        for m in ORDER:
            for dz in (1, -1):
                self.send(("ring", 1, m), self.blk(0, m), dz=dz)
        for m in ORDER:
            self.send("early", self.blk(0, m), other=True)

    def ring(self, k, m):
        self.got(("ring", k, m))
        if k < 4:
            for side in (-1, 1):
                part = None if k < 3 else (0 if side < 0 else 1)
                self.send(("ring", k + 1, m), self.blk(side * k, m, part), dz=-side)
            for side in (-1, 1):
                self.send("early" if k < 3 else ("late", m), self.blk(side * k, m), other=True)
        else:
            self.send(("late", m), self.blk(4, m), other=True)

    def far(self, k):
        self.got(("far", k))
        for dz in self.both(k):
            if k < 3 or (k == 3 and dz * self.flip > 0):
                self.send(("far", k + 1), self.one(dz, 0), dz=1 if dz < 0 else -1)
        self.cross_start(k, self.both(k))

    def cross(self, k):
        self.cross_on(k, self.both(k))

    def cross2(self, k):
        self.cross_end(k, self.both(k), "early" if k < 3 else ("late", 0))


def split(value):
    high = value.astype(BF)
    return high, (value - high.astype(F32)).astype(BF)


FLOOR = 2.0 ** -124


def coded(value):
    t = jnp.abs(value) * 8.0
    t = t * t
    t = t * t
    t = t * t * 2.0 ** 60
    t = jnp.maximum(t * t, FLOOR)
    return jnp.where(value < 0, -t, t).astype(BF)


def decoded(code):
    t = code.astype(F32)
    size = jnp.abs(t)
    root = jnp.exp(jnp.log(size) / 16.0) * (2.0 ** -7.5 / 8.0)
    root = jnp.where(size > FLOOR, root, 0.0)
    return jnp.where(t < 0, -root, root)


def dot(a, b):
    return lax.dot_general(a, b, (((1,), (0,)), ((), ())), preferred_element_type=F32)


def kernel(
    inputs, cots, factors, first, second, master,
    own_step, own_new, copy_v, fm, sm,
    xin, cin, ct, fw, mw, wide, gt, both_v, um, own_f32,
    pa, pb, ca, cb, sa, sb, rxa, rzb, ta, tb, rza, rxb, ga, gb, nn, squares, room,
    lsem, fs_sem, fr_sem, ms_sem, mr_sem, bs_sem, br_sem,
):
    z, x, c, y = (lax.axis_index(a) for a in ("z", "x", "c", "y"))
    pos = (z, x, c, y)

    local = []

    def load(src, dst):
        k = pltpu.make_async_copy(src, dst, lsem.at[len(local)])
        k.start()
        local.append(k)
        return k

    fl = [load(factors.at[pl.ds(0, 2), pl.ds(8 * q, 8), :], fw.at[pl.ds(0, 2), z, x, c, q]) for q in range(4)]
    fl.append(load(factors.at[2, pl.ds(pl.multiple_of(8 * y, 8), 8), :], fw.at[2, z, x, c, y]))
    ml = load(master, own_f32)
    cl = load(cots, cin)
    xl = load(inputs, xin)
    el = [load(first, fm), load(second, sm)]

    barrier = pltpu.get_barrier_semaphore()
    peers = []
    for dz in range(1, NZ):
        peers.append((lax.rem(z + dz, NZ), x, c, y))
    for dx in range(1, NX):
        peers.append((z, lax.rem(x + dx, NX), c, y))
    for dy in range(1, 4):
        peers.append((z, x, c, lax.rem(y + dy, 4)))
    peers.append((z, x, 1 - c, y))
    for peer in peers:
        pl.semaphore_signal(barrier, inc=1, device_id=peer, device_id_type=MESH)
    ml.wait()
    for m in range(3):
        mw[m, z, x, c] = coded(own_f32[m]).reshape(4, 8, 256)
    for k in fl:
        k.wait()
    pl.semaphore_wait(barrier, len(peers))

    def turned(m):
        ct[pl.ds(256 * m, 256), :] = cin[m].T

    def gradient(lo, hi):
        def body(zz, _):
            at = pl.ds(pl.multiple_of(zz * 256, 256), 256)
            g_hi, g_lo = split(dot(ct[...], xin[:, at]))
            for m in range(3):
                gt[m, zz, 0:256] = g_hi[256 * m:256 * (m + 1)]
                gt[m, zz, 256:512] = g_lo[256 * m:256 * (m + 1)]
            return 0
        lax.fori_loop(lo, hi, body, 0)

    f = Direct(pos, fw, fs_sem, fr_sem, room, -1, 8)
    w = Ring(pos, mw, ms_sem, mr_sem, room, 1, 16)
    r = Copies(pos, bs_sem, br_sem, room)

    def product(m, offsets):
        zs = [f.zof(dz) for dz in offsets]
        return dot(
            jnp.concatenate([gt[m, zz] for zz in zs], axis=1),
            jnp.concatenate([fw[m, zz].reshape(256, 256) for zz in zs], axis=0),
        )

    def project(m):
        if m == 2:
            both = product(m, range(8))
        else:
            both = both_v[m] + product(m, FAR_Z)
        part = (both[:256] + both[256:]).T
        for half in range(2):
            cols = part[:, half * 128:(half + 1) * 128]
            if m < 2:
                for xx in range(NX):
                    pa[half, m, xx] = cols[xx * 64:(xx + 1) * 64]
            else:
                for zz in range(NZ):
                    pb[half, zz] = cols[zz * 32:(zz + 1) * 32]

    zorder = (4, 3, -3, 2, -2, 1, -1)
    xorder = (2, 1, -1)

    def widen(m):
        def body(zz, _):
            at = pl.ds(pl.multiple_of(m * D + zz * 256, 256), 256)
            wide[at, :] = decoded(mw[m, zz].reshape(256, 256))
            return 0
        lax.fori_loop(0, NZ, body, 0)

    def moments(m):
        for half in range(2):
            cols = slice(half * 128, (half + 1) * 128)
            if m < 2:
                proj = jnp.concatenate([ga[half, m, xx, zz] for xx in range(NX) for zz in range(NZ)], axis=0)
            else:
                proj = jnp.concatenate([gb[half, zz, xx] for zz in range(NZ) for xx in range(NX)], axis=0)
            nf = beta_first * fm[m, :, cols] + (1.0 - beta_first) * proj
            ns = beta_second * sm[m, :, cols] + (1.0 - beta_second) * proj * proj
            fm[m, :, cols] = nf
            sm[m, :, cols] = ns
            hi, lo = split(nf / (jnp.sqrt(ns) + adam_eps))
            nn[m, 0:256, cols] = hi
            nn[m, 256:512, cols] = lo

    def update(m):
        def body(zz, acc):
            fz = fw[m, pl.ds(4 * zz, 4)].reshape(1024, 256)
            u = dot(jnp.concatenate([fz, fz], axis=1), nn[m])
            um[m, pl.ds(pl.multiple_of(zz * 1024, 1024), 1024), :] = u
            uu = jnp.sum((u * u).reshape(128, 8, 256), axis=0)
            return acc + uu[:, :128] + uu[:, 128:]
        squares[y, m] = lax.fori_loop(0, 2, body, jnp.zeros((8, 128), F32))
        for dy in (1, 2, 3):
            r.send(("ys", m), squares.at[y, m], dy=dy)

    f.start()
    cl.wait()
    for m in range(3):
        turned(m)
    xl.wait()
    gradient(0, 2)
    f.quarter()
    f.near()
    f.far(1, NEAR_Z)
    gradient(2, 4)
    f.line_end(0, (0,), "early")
    f.far(2, FAR_Z)
    gradient(4, 6)
    f.columns()
    gradient(6, 8)
    f.ring(1, NEAR_Z, "early")
    w.start()
    f.line_end(1, NEAR_Z, "early")
    f.ring(2, FAR_Z, "late")
    f.line_end(2, FAR_Z, "late")
    f.got("early")
    for m in range(2):
        both_v[m] = product(m, (0,) + NEAR_Z)
    f.exchange()
    w.far(1)
    w.cross(0)
    w.near()
    f.got("late")
    for m in range(2):
        project(m)
        r.send(("k", m), pa.at[1 - c, m], ca.at[m], other=True)
    f.got("last")
    project(2)
    r.send(("k", 2), pb.at[1 - c], cb, other=True)
    for m in range(2):
        r.got(("k", m))
        sa[m] = pa[c, m] + ca[m]
        for i, dx in enumerate(xorder):
            r.send(("a1", m), sa.at[m, r.xof(dx)], rxa.at[m, i], dx=dx)
    r.got(("k", 2))
    sb[...] = pb[c] + cb[...]
    for i, dz in enumerate(zorder):
        r.send("b1", sb.at[r.zof(dz)], rzb.at[i], dz=dz)
    w.far(2)
    w.cross(1)
    w.cross2(0)
    for m in ORDER:
        w.ring(1, m)
    for m in range(2):
        r.got(("a1", m))
        tot = sa[m, x]
        for i in range(3):
            tot = tot + rxa[m, i]
        for zz in range(NZ):
            ta[m, zz] = tot[zz * 8:(zz + 1) * 8]
        for i, dz in enumerate(zorder):
            r.send(("a2", m), ta.at[m, r.zof(dz)], rza.at[m, i], dz=dz)
    w.far(3)
    w.cross(2)
    w.cross2(1)
    r.got("b1")
    tot = sb[z]
    for i in range(7):
        tot = tot + rzb[i]
    for xx in range(NX):
        tb[xx] = tot[xx * 8:(xx + 1) * 8]
    for i, dx in enumerate(xorder):
        r.send("b2", tb.at[r.xof(dx)], rxb.at[i], dx=dx)
    for m in ORDER:
        w.ring(2, m)
    for m in range(2):
        r.got(("a2", m))
        tot = ta[m, z]
        for i in range(7):
            tot = tot + rza[m, i]
        ga[c, m, x, z] = tot
        for dz in zorder:
            r.send(("a3", m), ga.at[c, m, x, z], dz=dz)
    r.got("b2")
    tot = tb[x]
    for i in range(3):
        tot = tot + rxb[i]
    gb[c, z, x] = tot
    for dx in xorder:
        r.send("b3", gb.at[c, z, x], dx=dx)
    w.far(4)
    w.cross(3)
    w.cross2(2)
    for m in ORDER:
        w.ring(3, m)
    r.got("b3")
    for dz in zorder:
        r.send("b4", gb.at[c, z], dz=dz)
    for m in range(2):
        r.got(("a3", m))
        for dx in xorder:
            r.send(("a4", m), ga.at[c, m, x], dx=dx)
        r.send(("ka", m), ga.at[c, m, x], other=True)
    for k in el:
        k.wait()
    w.cross(4)
    w.cross2(3)
    for m in ORDER:
        w.ring(4, m)
    for m in range(2):
        r.got(("a4", m))
        for dx in xorder:
            r.send(("ka", m), ga.at[c, m, r.xof(-dx)], other=True)
    r.got("b4")
    r.send("kb", gb.at[c], other=True)
    w.cross2(4)
    for m in range(2):
        r.got(("ka", m))
        moments(m)
        update(m)
    r.got("kb")
    moments(2)
    update(2)
    w.got("early")
    for m in ORDER:
        w.got(("late", m))
        widen(m)

    rows = pl.multiple_of(z * 256 + x * 64 + c * 32, 32)
    for m in ORDER:
        r.got(("ys", m))
        tot = squares[0, m]
        for j in range(1, 4):
            tot = tot + squares[j, m]
        inv = 1.0 / jnp.sqrt(jnp.sum(tot, keepdims=True) / (D * MW) + norm_eps)
        step = um[m, pl.ds(rows, 32), :] * inv
        own_step[m] = step
        own_new[m] = own_f32[m] - learning_rate * step

        def body(zz, _):
            at = pl.ds(pl.multiple_of(zz * 256, 256), 256)
            copy_v[m, at, :] = (wide[pl.ds(pl.multiple_of(m * D + zz * 256, 256), 256), :] - learning_rate * (um[m, at, :] * inv)).astype(BF)
            return 0
        lax.fori_loop(0, NZ, body, 0)
    f.drain()
    w.drain()
    r.drain()


def write_out(*refs):
    sem = refs[-1]
    copies = []
    for i in (2, 3, 4, 0, 1):
        for m in range(3):
            copies.append(pltpu.make_async_copy(refs[i].at[m], refs[5 + i].at[m], sem.at[len(copies)]))
    for k in copies:
        k.start()
    for k in copies:
        k.wait()


def local(inputs, cotangents, factors, first_moment, second_moment, master):
    cots = jnp.transpose(cotangents, (1, 0, 2))
    hbm = pl.BlockSpec(memory_space=pltpu.HBM)
    V = pltpu.VMEM
    dma = pltpu.SemaphoreType.DMA
    results = pl.pallas_call(
        kernel,
        out_shape=(
            V((3, 32, 256), F32), V((3, 32, 256), F32), V((3, D, 256), BF), V((3, 256, 256), F32), V((3, 256, 256), F32),
        ),
        in_specs=[hbm] * 6,
        out_specs=(pl.BlockSpec(memory_space=pltpu.VMEM),) * 5,
        scratch_shapes=[
            V((1024, 2048), BF), V((3, 1024, 256), BF), V((768, 1024), BF),
            V((3, NZ, NX, 2, 4, 8, 256), BF), V((3, NZ, NX, 2, 4, 8, 256), BF), V((3 * D, 256), F32),
            V((3, NZ, 512, 256), BF), V((3, 512, 256), F32), V((3, D, 256), F32), V((3, 32, 256), F32),
            V((2, 2, NX, 64, 128), F32), V((2, NZ, 32, 128), F32),
            V((2, NX, 64, 128), F32), V((NZ, 32, 128), F32),
            V((2, NX, 64, 128), F32), V((NZ, 32, 128), F32),
            V((2, 3, 64, 128), F32), V((7, 32, 128), F32),
            V((2, NZ, 8, 128), F32), V((NX, 8, 128), F32),
            V((2, 7, 8, 128), F32), V((3, 8, 128), F32),
            V((2, 2, NX, NZ, 8, 128), F32), V((2, NZ, NX, 8, 128), F32),
            V((3, 512, 256), BF), V((4, 3, 8, 128), F32), V((1024, 8, 128), F32),
            dma((16,)),
            dma((1,)), dma((GROUPS,)), dma((1,)), dma((GROUPS,)),
            dma((1,)), dma((GROUPS,)),
        ],
        compiler_params=pltpu.CompilerParams(collective_id=0, has_side_effects=True, vmem_limit_bytes=58 * 1024 * 1024),
        name="update",
    )(inputs, cots, factors, first_moment, second_moment, master)
    return pl.pallas_call(
        write_out,
        out_shape=tuple(jax.ShapeDtypeStruct(r.shape, r.dtype) for r in results),
        in_specs=[pl.BlockSpec(memory_space=pl.ANY)] * 5,
        out_specs=(hbm,) * 5,
        scratch_shapes=[dma((15,))],
        compiler_params=pltpu.CompilerParams(vmem_limit_bytes=1024 * 1024),
        name="write_out",
    )(*results)


def solution(mesh):
    torus = Mesh(mesh.devices.reshape(NZ, NX, 2, mesh.shape["tp"]), ("z", "x", "c", "y"))
    fs = ("z", "x", "c")
    return jax.shard_map(
        local,
        mesh=torus,
        in_specs=(
            P(fs, None),
            P(fs, None, "y"),
            P(None, fs, None),
            P(None, None, "y"),
            P(None, None, "y"),
            P(None, fs, "y"),
        ),
        out_specs=(
            P(None, fs, "y"),
            P(None, fs, "y"),
            P(None, None, "y"),
            P(None, None, "y"),
            P(None, None, "y"),
        ),
        check_vma=False,
    )
```

```python
import math

import jax
import jax.numpy as jnp
from jax import lax
from jax.experimental import pallas as pl
from jax.experimental.pallas import tpu as pltpu
from jax.sharding import Mesh
from jax.sharding import PartitionSpec as P

D = 2048
MW = 1024
BF = jnp.bfloat16
F32 = jnp.float32
MESH = pl.DeviceIdType.MESH

beta_first = 0.8
beta_second = 0.9
adam_eps = 1e-08
norm_eps = 1e-06
learning_rate = 0.005

NZ, NX = 8, 4
GROUPS = 40
ORDER = (0, 1, 2)


class Copies:
    def __init__(self, pos, ssem, rsem, room):
        self.z, self.x, self.c, self.y = pos
        self.ssem, self.rsem, self.room = ssem, rsem, room
        self.sent = 0
        self.groups = {}

    def zof(self, dz):
        return lax.rem(self.z + (dz + NZ), NZ)

    def xof(self, dx):
        return lax.rem(self.x + (dx + NX), NX)

    def send(self, key, src, dst=None, dz=0, dx=0, dy=0, other=False):
        dst = src if dst is None else dst
        if key not in self.groups:
            self.groups[key] = [len(self.groups), 0]
        group = self.groups[key]
        size = math.prod(src.shape) * jnp.dtype(src.dtype).itemsize
        group[1] += size
        self.sent += size
        pltpu.make_async_remote_copy(
            src_ref=src, dst_ref=dst, send_sem=self.ssem.at[0], recv_sem=self.rsem.at[group[0]],
            device_id=(self.zof(dz), self.xof(dx), 1 - self.c if other else self.c, lax.rem(self.y + dy, 4)), device_id_type=MESH,
        ).start()

    def bytes_at(self, sem, size):
        part = self.room.at[pl.ds(0, size // 4096)]
        pltpu.make_async_copy(part, part, sem).wait()

    def got(self, key):
        self.bytes_at(self.rsem.at[self.groups[key][0]], self.groups[key][1])

    def drain(self):
        self.bytes_at(self.ssem.at[0], self.sent)


class Gather(Copies):
    def __init__(self, pos, whole, ssem, rsem, room, flip, rows):
        super().__init__(pos, ssem, rsem, room)
        self.b = whole
        self.flip = flip
        self.q0, self.q1 = pl.ds(0, rows // 8), pl.ds(rows // 8, 4 - rows // 8)

    def blk(self, dz, m, part=None):
        xs = slice(None) if part is None else pl.ds(2 * part, 2)
        return self.b.at[m, self.zof(dz), xs, self.c, self.q0]

    def one(self, dz, dx):
        return self.b.at[:, self.zof(dz), self.xof(dx), self.c, self.q1]

    def line(self, dz):
        return self.b.at[:, self.zof(dz), :, self.c, self.q1]

    def start_x(self):
        own = self.b.at[:, self.z, self.x, self.c, self.q0]
        for dx in (2, 1, -1):
            self.send("near", own, dx=dx)

    def cross_start(self, k, offsets):
        for dz in offsets:
            for dx in (1, -1):
                self.send(("cross", k), self.one(dz, 0), dx=dx)

    def cross_on(self, k, offsets):
        self.got(("cross", k))
        for dz in offsets:
            side = self.flip if dz % 2 else -self.flip
            self.send(("cross2", k), self.one(dz, side), dx=-side)

    def cross_end(self, k, offsets, key):
        self.got(("cross2", k))
        for dz in offsets:
            self.send(key, self.line(dz), other=True)


NEAR_Z, FAR_Z = (1, -1, 2, -2), (3, -3, 4)


class Direct(Gather):
    def own0(self):
        return self.b.at[pl.ds(0, 2), self.z, :, self.c, self.q0]

    def one(self, dz, dx):
        return self.b.at[pl.ds(0, 2), self.zof(dz), self.xof(dx), self.c, self.q1]

    def line(self, dz):
        return self.b.at[pl.ds(0, 2), self.zof(dz), :, self.c, self.q1]

    def column(self, dx):
        return self.b.at[2, :, self.xof(dx), self.c, self.y]

    def start(self):
        own = self.b.at[pl.ds(0, 2), self.z, self.x, self.c, self.q0]
        for dx in (2, 1, -1):
            self.send("near", own, dx=dx)
        own = self.b.at[2, self.z, self.x, self.c, self.y]
        for dz in FAR_Z + NEAR_Z:
            self.send("quarter", own, dz=dz)
        for dz in NEAR_Z:
            self.send(("far", 1), self.one(0, 0), dz=dz)
        self.line_start(0, (0,))
        for dz in FAR_Z:
            self.send(("far", 2), self.one(0, 0), dz=dz)

    def line_start(self, k, offsets):
        for dz in offsets:
            for dx in (2, 1, -1):
                self.send(("cross", k), self.one(dz, 0), dx=dx)

    def near(self):
        self.got("near")
        for k, offsets in ((1, NEAR_Z), (2, FAR_Z)):
            for dz in offsets:
                self.send(("ring", k), self.own0(), dz=dz)
        self.send("early", self.own0(), other=True)

    def quarter(self):
        self.got("quarter")
        for dx in (2, 1, -1):
            self.send("columns", self.column(0), dx=dx)
        for dy in (2, 1, 3):
            self.send("exchange", self.column(0), dy=dy)

    def columns(self):
        self.got("columns")
        for dx in (1, -1, 2):
            for dy in (2, 1, 3):
                self.send("exchange", self.column(dx), dy=dy)
        self.send("last", self.b.at[2, :, :, self.c, self.y], other=True)

    def exchange(self):
        self.got("exchange")
        for dy in (1, 2, 3):
            self.send("last", self.b.at[2, :, :, self.c, lax.rem(self.y + dy, 4)], other=True)

    def ring(self, k, offsets, key):
        self.got(("ring", k))
        for dz in offsets:
            self.send(key, self.b.at[pl.ds(0, 2), self.zof(dz), :, self.c, self.q0], other=True)

    def far(self, k, offsets):
        self.got(("far", k))
        self.line_start(k, offsets)

    def line_end(self, k, offsets, key):
        self.got(("cross", k))
        for dz in offsets:
            self.send(key, self.line(dz), other=True)


class Ring(Gather):
    def both(self, k):
        return (k, -k) if 0 < k < 4 else (self.flip * k,)

    def start(self):
        self.start_x()
        for dz in (1, -1):
            self.send(("far", 1), self.one(0, 0), dz=dz)
        self.cross_start(0, (0,))

    def near(self):
        self.got("near")
        for m in ORDER:
            for dz in (1, -1):
                self.send(("ring", 1, m), self.blk(0, m), dz=dz)
        for m in ORDER:
            self.send("early", self.blk(0, m), other=True)

    def ring(self, k, m):
        self.got(("ring", k, m))
        if k < 4:
            for side in (-1, 1):
                part = None if k < 3 else (0 if side < 0 else 1)
                self.send(("ring", k + 1, m), self.blk(side * k, m, part), dz=-side)
            for side in (-1, 1):
                self.send("early" if k < 3 else ("late", m), self.blk(side * k, m), other=True)
        else:
            self.send(("late", m), self.blk(4, m), other=True)

    def far(self, k):
        self.got(("far", k))
        for dz in self.both(k):
            if k < 3 or (k == 3 and dz * self.flip > 0):
                self.send(("far", k + 1), self.one(dz, 0), dz=1 if dz < 0 else -1)
        self.cross_start(k, self.both(k))

    def cross(self, k):
        self.cross_on(k, self.both(k))

    def cross2(self, k):
        self.cross_end(k, self.both(k), "early" if k < 3 else ("late", 0))


def split(value):
    high = value.astype(BF)
    return high, (value - high.astype(F32)).astype(BF)


CODE_SCALE, CODE_SHIFT = 250.0 / math.sqrt(0.125), 125.0


def coded(value):
    t = jnp.exp2(jnp.sqrt(jnp.abs(value)) * CODE_SCALE - CODE_SHIFT)
    return jnp.where(value < 0, -t, t).astype(BF)


def decoded(code):
    t = code.astype(F32)
    root = jnp.log(jnp.abs(t)) * (1.0 / (math.log(2.0) * CODE_SCALE)) + CODE_SHIFT / CODE_SCALE
    size = root * root
    return jnp.where(t < 0, -size, size)


def dot(a, b):
    return lax.dot_general(a, b, (((1,), (0,)), ((), ())), preferred_element_type=F32)


def kernel(
    inputs, cots, factors, first, second, master,
    own_step, own_new, copy_v, fm, sm,
    xin, cin, ct, fw, mw, wide, gt, both_v, um, own_f32,
    pa, pb, ca, cb, sa, sb, rxa, rzb, ta, tb, rza, rxb, ga, gb, nn, squares, room,
    lsem, fs_sem, fr_sem, ms_sem, mr_sem, bs_sem, br_sem,
):
    z, x, c, y = (lax.axis_index(a) for a in ("z", "x", "c", "y"))
    pos = (z, x, c, y)

    barrier = pltpu.get_barrier_semaphore()
    peers = []
    for dz in range(1, NZ):
        peers.append((lax.rem(z + dz, NZ), x, c, y))
    for dx in range(1, NX):
        peers.append((z, lax.rem(x + dx, NX), c, y))
    for dy in range(1, 4):
        peers.append((z, x, c, lax.rem(y + dy, 4)))
    peers.append((z, x, 1 - c, y))
    for peer in peers:
        pl.semaphore_signal(barrier, inc=1, device_id=peer, device_id_type=MESH)
    local = []

    def load(src, dst):
        k = pltpu.make_async_copy(src, dst, lsem.at[len(local)])
        k.start()
        local.append(k)
        return k

    fl = [load(factors.at[pl.ds(0, 2), pl.ds(8 * q, 8), :], fw.at[pl.ds(0, 2), z, x, c, q]) for q in range(4)]
    fl.append(load(factors.at[2, pl.ds(pl.multiple_of(8 * y, 8), 8), :], fw.at[2, z, x, c, y]))
    ml = load(master, own_f32)
    cl = load(cots, cin)
    xl = load(inputs, xin)
    el = [load(first, fm), load(second, sm)]

    ml.wait()
    for m in range(3):
        mw[m, z, x, c] = coded(own_f32[m]).reshape(4, 8, 256)
    for k in fl:
        k.wait()
    pl.semaphore_wait(barrier, len(peers))

    def turned(m):
        ct[pl.ds(256 * m, 256), :] = cin[m].T

    def gradient(lo, hi):
        def body(zz, _):
            at = pl.ds(pl.multiple_of(zz * 256, 256), 256)
            g_hi, g_lo = split(dot(ct[...], xin[:, at]))
            for m in range(3):
                gt[m, zz, 0:256] = g_hi[256 * m:256 * (m + 1)]
                gt[m, zz, 256:512] = g_lo[256 * m:256 * (m + 1)]
            return 0
        lax.fori_loop(lo, hi, body, 0)

    f = Direct(pos, fw, fs_sem, fr_sem, room, -1, 8)
    w = Ring(pos, mw, ms_sem, mr_sem, room, 1, 8)
    r = Copies(pos, bs_sem, br_sem, room)

    def product(m, offsets):
        zs = [f.zof(dz) for dz in offsets]
        return dot(
            jnp.concatenate([gt[m, zz] for zz in zs], axis=1),
            jnp.concatenate([fw[m, zz].reshape(256, 256) for zz in zs], axis=0),
        )

    def project(m):
        if m == 2:
            both = product(m, range(8))
        else:
            both = both_v[m] + product(m, FAR_Z)
        part = (both[:256] + both[256:]).T
        for half in range(2):
            cols = part[:, half * 128:(half + 1) * 128]
            if m < 2:
                for xx in range(NX):
                    pa[half, m, xx] = cols[xx * 64:(xx + 1) * 64]
            else:
                for zz in range(NZ):
                    pb[half, zz] = cols[zz * 32:(zz + 1) * 32]

    zorder = (4, 3, -3, 2, -2, 1, -1)
    xorder = (2, 1, -1)

    def widen(m):
        def body(zz, _):
            at = pl.ds(pl.multiple_of(m * D + zz * 256, 256), 256)
            wide[at, :] = decoded(mw[m, zz].reshape(256, 256))
            return 0
        lax.fori_loop(0, NZ, body, 0)

    def moments(m):
        for half in range(2):
            cols = slice(half * 128, (half + 1) * 128)
            if m < 2:
                proj = jnp.concatenate([ga[half, m, xx, zz] for xx in range(NX) for zz in range(NZ)], axis=0)
            else:
                proj = jnp.concatenate([gb[half, zz, xx] for zz in range(NZ) for xx in range(NX)], axis=0)
            nf = beta_first * fm[m, :, cols] + (1.0 - beta_first) * proj
            ns = beta_second * sm[m, :, cols] + (1.0 - beta_second) * proj * proj
            fm[m, :, cols] = nf
            sm[m, :, cols] = ns
            hi, lo = split(nf / (jnp.sqrt(ns) + adam_eps))
            nn[m, 0:256, cols] = hi
            nn[m, 256:512, cols] = lo

    def update(m):
        def body(zz, acc):
            fz = fw[m, pl.ds(4 * zz, 4)].reshape(1024, 256)
            u = dot(jnp.concatenate([fz, fz], axis=1), nn[m])
            um[m, pl.ds(pl.multiple_of(zz * 1024, 1024), 1024), :] = u
            uu = jnp.sum((u * u).reshape(128, 8, 256), axis=0)
            return acc + uu[:, :128] + uu[:, 128:]
        squares[y, m] = lax.fori_loop(0, 2, body, jnp.zeros((8, 128), F32))
        for dy in (1, 2, 3):
            r.send(("ys", m), squares.at[y, m], dy=dy)

    f.start()
    cl.wait()
    for m in range(3):
        turned(m)
    xl.wait()
    gradient(0, 2)
    f.near()
    f.quarter()
    f.far(1, NEAR_Z)
    gradient(2, 4)
    f.line_end(0, (0,), "early")
    f.far(2, FAR_Z)
    gradient(4, 6)
    f.columns()
    gradient(6, 8)
    f.ring(1, NEAR_Z, "early")
    w.start()
    f.line_end(1, NEAR_Z, "early")
    f.ring(2, FAR_Z, "late")
    f.line_end(2, FAR_Z, "late")
    f.got("early")
    for m in range(2):
        both_v[m] = product(m, (0,) + NEAR_Z)
    f.exchange()
    w.far(1)
    w.cross(0)
    w.near()
    f.got("late")
    for m in range(2):
        project(m)
        r.send(("k", m), pa.at[1 - c, m], ca.at[m], other=True)

    def reduce_a1(m):
        r.got(("k", m))
        sa[m] = pa[c, m] + ca[m]
        for i, dx in enumerate(xorder):
            r.send(("a1", m), sa.at[m, r.xof(dx)], rxa.at[m, i], dx=dx)

    f.got("last")
    reduce_a1(0)
    project(2)
    r.send(("k", 2), pb.at[1 - c], cb, other=True)
    reduce_a1(1)
    r.got(("k", 2))
    sb[...] = pb[c] + cb[...]
    for i, dz in enumerate(zorder):
        r.send("b1", sb.at[r.zof(dz)], rzb.at[i], dz=dz)
    w.far(2)
    w.cross(1)
    w.cross2(0)
    for m in range(2):
        r.got(("a1", m))
        tot = sa[m, x]
        for i in range(3):
            tot = tot + rxa[m, i]
        for zz in range(NZ):
            ta[m, zz] = tot[zz * 8:(zz + 1) * 8]
        for i, dz in enumerate(zorder):
            r.send(("a2", m), ta.at[m, r.zof(dz)], rza.at[m, i], dz=dz)
    r.got("b1")
    tot = sb[z]
    for i in range(7):
        tot = tot + rzb[i]
    for xx in range(NX):
        tb[xx] = tot[xx * 8:(xx + 1) * 8]
    for i, dx in enumerate(xorder):
        r.send("b2", tb.at[r.xof(dx)], rxb.at[i], dx=dx)
    for m in ORDER:
        w.ring(1, m)
    w.far(3)
    w.cross(2)
    w.cross2(1)
    for m in range(2):
        r.got(("a2", m))
        tot = ta[m, z]
        for i in range(7):
            tot = tot + rza[m, i]
        ga[c, m, x, z] = tot
        for dz in zorder:
            r.send(("a3", m), ga.at[c, m, x, z], dz=dz)
    r.got("b2")
    tot = tb[x]
    for i in range(3):
        tot = tot + rxb[i]
    gb[c, z, x] = tot
    for dx in xorder:
        r.send("b3", gb.at[c, z, x], dx=dx)
    for m in ORDER:
        w.ring(2, m)
    w.far(4)
    w.cross(3)
    w.cross2(2)
    r.got("b3")
    for dz in zorder:
        r.send("b4", gb.at[c, z], dz=dz)
    for m in range(2):
        r.got(("a3", m))
        for dx in xorder:
            r.send(("a4", m), ga.at[c, m, x], dx=dx)
        r.send(("ka", m), ga.at[c, m, x], other=True)
    for k in el:
        k.wait()
    for m in ORDER:
        w.ring(3, m)
    w.cross(4)
    w.cross2(3)
    for m in range(2):
        r.got(("a4", m))
        for dx in xorder:
            r.send(("ka", m), ga.at[c, m, r.xof(-dx)], other=True)
    r.got("b4")
    r.send("kb", gb.at[c], other=True)
    w.cross2(4)
    for m in ORDER:
        w.ring(4, m)
    for m in range(2):
        r.got(("ka", m))
        moments(m)
        update(m)
    r.got("kb")
    moments(2)
    update(2)
    w.got("early")
    for m in ORDER:
        w.got(("late", m))
        widen(m)

    rows = pl.multiple_of(z * 256 + x * 64 + c * 32, 32)
    for m in ORDER:
        r.got(("ys", m))
        tot = squares[0, m]
        for j in range(1, 4):
            tot = tot + squares[j, m]
        inv = 1.0 / jnp.sqrt(jnp.sum(tot, keepdims=True) / (D * MW) + norm_eps)
        step = um[m, pl.ds(rows, 32), :] * inv
        own_step[m] = step
        own_new[m] = own_f32[m] - learning_rate * step

        def body(zz, _):
            at = pl.ds(pl.multiple_of(zz * 256, 256), 256)
            copy_v[m, at, :] = (wide[pl.ds(pl.multiple_of(m * D + zz * 256, 256), 256), :] - learning_rate * (um[m, at, :] * inv)).astype(BF)
            return 0
        lax.fori_loop(0, NZ, body, 0)
    f.drain()
    w.drain()
    r.drain()


def write_out(*refs):
    sem = refs[-1]
    copies = []
    for i in (2, 3, 4, 0, 1):
        for m in range(3):
            copies.append(pltpu.make_async_copy(refs[i].at[m], refs[5 + i].at[m], sem.at[len(copies)]))
    for k in copies:
        k.start()
    for k in copies:
        k.wait()


def local(inputs, cotangents, factors, first_moment, second_moment, master):
    cots = jnp.transpose(cotangents, (1, 0, 2))
    hbm = pl.BlockSpec(memory_space=pltpu.HBM)
    V = pltpu.VMEM
    dma = pltpu.SemaphoreType.DMA
    results = pl.pallas_call(
        kernel,
        out_shape=(
            V((3, 32, 256), F32), V((3, 32, 256), F32), V((3, D, 256), BF), V((3, 256, 256), F32), V((3, 256, 256), F32),
        ),
        in_specs=[hbm] * 6,
        out_specs=(pl.BlockSpec(memory_space=pltpu.VMEM),) * 5,
        scratch_shapes=[
            V((1024, 2048), BF), V((3, 1024, 256), BF), V((768, 1024), BF),
            V((3, NZ, NX, 2, 4, 8, 256), BF), V((3, NZ, NX, 2, 4, 8, 256), BF), V((3 * D, 256), F32),
            V((3, NZ, 512, 256), BF), V((3, 512, 256), F32), V((3, D, 256), F32), V((3, 32, 256), F32),
            V((2, 2, NX, 64, 128), F32), V((2, NZ, 32, 128), F32),
            V((2, NX, 64, 128), F32), V((NZ, 32, 128), F32),
            V((2, NX, 64, 128), F32), V((NZ, 32, 128), F32),
            V((2, 3, 64, 128), F32), V((7, 32, 128), F32),
            V((2, NZ, 8, 128), F32), V((NX, 8, 128), F32),
            V((2, 7, 8, 128), F32), V((3, 8, 128), F32),
            V((2, 2, NX, NZ, 8, 128), F32), V((2, NZ, NX, 8, 128), F32),
            V((3, 512, 256), BF), V((4, 3, 8, 128), F32), V((1024, 8, 128), F32),
            dma((16,)),
            dma((1,)), dma((GROUPS,)), dma((1,)), dma((GROUPS,)),
            dma((1,)), dma((GROUPS,)),
        ],
        compiler_params=pltpu.CompilerParams(collective_id=0, has_side_effects=True, vmem_limit_bytes=58 * 1024 * 1024),
        name="update",
    )(inputs, cots, factors, first_moment, second_moment, master)
    return pl.pallas_call(
        write_out,
        out_shape=tuple(jax.ShapeDtypeStruct(r.shape, r.dtype) for r in results),
        in_specs=[pl.BlockSpec(memory_space=pl.ANY)] * 5,
        out_specs=(hbm,) * 5,
        scratch_shapes=[dma((15,))],
        compiler_params=pltpu.CompilerParams(vmem_limit_bytes=1024 * 1024),
        name="write_out",
    )(*results)


def solution(mesh):
    torus = Mesh(mesh.devices.reshape(NZ, NX, 2, mesh.shape["tp"]), ("z", "x", "c", "y"))
    fs = ("z", "x", "c")
    return jax.shard_map(
        local,
        mesh=torus,
        in_specs=(
            P(fs, None),
            P(fs, None, "y"),
            P(None, fs, None),
            P(None, None, "y"),
            P(None, None, "y"),
            P(None, fs, "y"),
        ),
        out_specs=(
            P(None, fs, "y"),
            P(None, fs, "y"),
            P(None, None, "y"),
            P(None, None, "y"),
            P(None, None, "y"),
        ),
        check_vma=False,
    )
```

```python
import math

import jax
import jax.numpy as jnp
from jax import lax
from jax.experimental import pallas as pl
from jax.experimental.pallas import tpu as pltpu
from jax.sharding import Mesh
from jax.sharding import PartitionSpec as P

D = 2048
MW = 1024
BF = jnp.bfloat16
F32 = jnp.float32
MESH = pl.DeviceIdType.MESH

beta_first = 0.8
beta_second = 0.9
adam_eps = 1e-08
norm_eps = 1e-06
learning_rate = 0.005

NZ, NX = 8, 4
GROUPS = 40
ORDER = (0, 1, 2)


class Copies:
    def __init__(self, pos, ssem, rsem, room):
        self.z, self.x, self.c, self.y = pos
        self.ssem, self.rsem, self.room = ssem, rsem, room
        self.sent = 0
        self.groups = {}

    def zof(self, dz):
        return lax.rem(self.z + (dz + NZ), NZ)

    def xof(self, dx):
        return lax.rem(self.x + (dx + NX), NX)

    def send(self, key, src, dst=None, dz=0, dx=0, dy=0, other=False):
        dst = src if dst is None else dst
        if key not in self.groups:
            self.groups[key] = [len(self.groups), 0]
        group = self.groups[key]
        size = math.prod(src.shape) * jnp.dtype(src.dtype).itemsize
        group[1] += size
        self.sent += size
        pltpu.make_async_remote_copy(
            src_ref=src, dst_ref=dst, send_sem=self.ssem.at[0], recv_sem=self.rsem.at[group[0]],
            device_id=(self.zof(dz), self.xof(dx), 1 - self.c if other else self.c, lax.rem(self.y + dy, 4)), device_id_type=MESH,
        ).start()

    def bytes_at(self, sem, size):
        part = self.room.at[pl.ds(0, size // 4096)]
        pltpu.make_async_copy(part, part, sem).wait()

    def got(self, key):
        self.bytes_at(self.rsem.at[self.groups[key][0]], self.groups[key][1])

    def drain(self):
        self.bytes_at(self.ssem.at[0], self.sent)


class Gather(Copies):
    def __init__(self, pos, whole, ssem, rsem, room, flip, rows):
        super().__init__(pos, ssem, rsem, room)
        self.b = whole
        self.flip = flip
        self.q0, self.q1 = pl.ds(0, rows // 8), pl.ds(rows // 8, 4 - rows // 8)

    def blk(self, dz, m, part=None):
        xs = slice(None) if part is None else pl.ds(2 * part, 2)
        return self.b.at[m, self.zof(dz), xs, self.c, self.q0]

    def one(self, dz, dx):
        return self.b.at[:, self.zof(dz), self.xof(dx), self.c, self.q1]

    def line(self, dz):
        return self.b.at[:, self.zof(dz), :, self.c, self.q1]

    def start_x(self):
        own = self.b.at[:, self.z, self.x, self.c, self.q0]
        for dx in (2, 1, -1):
            self.send("near", own, dx=dx)

    def cross_start(self, k, offsets):
        for dz in offsets:
            for dx in (1, -1):
                self.send(("cross", k), self.one(dz, 0), dx=dx)

    def cross_on(self, k, offsets):
        self.got(("cross", k))
        for dz in offsets:
            side = self.flip if dz % 2 else -self.flip
            self.send(("cross2", k), self.one(dz, side), dx=-side)

    def cross_end(self, k, offsets, key):
        self.got(("cross2", k))
        for dz in offsets:
            self.send(key, self.line(dz), other=True)


NEAR_Z, FAR_Z = (1, -1, 2, -2), (3, -3, 4)


class Direct(Gather):
    def own0(self):
        return self.b.at[pl.ds(0, 2), self.z, :, self.c, self.q0]

    def one(self, dz, dx):
        return self.b.at[pl.ds(0, 2), self.zof(dz), self.xof(dx), self.c, self.q1]

    def line(self, dz):
        return self.b.at[pl.ds(0, 2), self.zof(dz), :, self.c, self.q1]

    def column(self, dx):
        return self.b.at[2, :, self.xof(dx), self.c, self.y]

    def start(self):
        own = self.b.at[pl.ds(0, 2), self.z, self.x, self.c, self.q0]
        for dx in (2, 1, -1):
            self.send("near", own, dx=dx)
        own = self.b.at[2, self.z, self.x, self.c, self.y]
        for dz in FAR_Z + NEAR_Z:
            self.send("quarter", own, dz=dz)
        for dz in NEAR_Z:
            self.send(("far", 1), self.one(0, 0), dz=dz)
        self.line_start(0, (0,))
        for dz in FAR_Z:
            self.send(("far", 2), self.one(0, 0), dz=dz)

    def line_start(self, k, offsets):
        for dz in offsets:
            for dx in (2, 1, -1):
                self.send(("cross", k), self.one(dz, 0), dx=dx)

    def near(self):
        self.got("near")
        for k, offsets in ((1, NEAR_Z), (2, FAR_Z)):
            for dz in offsets:
                self.send(("ring", k), self.own0(), dz=dz)
        self.send("early", self.own0(), other=True)

    def quarter(self):
        self.got("quarter")
        for dx in (2, 1, -1):
            self.send("columns", self.column(0), dx=dx)
        for dy in (2, 1, 3):
            self.send("exchange", self.column(0), dy=dy)

    def columns(self):
        self.got("columns")
        for dx in (1, -1, 2):
            for dy in (2, 1, 3):
                self.send("exchange", self.column(dx), dy=dy)
        self.send("last", self.b.at[2, :, :, self.c, self.y], other=True)

    def exchange(self):
        self.got("exchange")
        for dy in (1, 2, 3):
            self.send("last", self.b.at[2, :, :, self.c, lax.rem(self.y + dy, 4)], other=True)

    def ring(self, k, offsets, key):
        self.got(("ring", k))
        for dz in offsets:
            self.send(key, self.b.at[pl.ds(0, 2), self.zof(dz), :, self.c, self.q0], other=True)

    def far(self, k, offsets):
        self.got(("far", k))
        self.line_start(k, offsets)

    def line_end(self, k, offsets, key):
        self.got(("cross", k))
        for dz in offsets:
            self.send(key, self.line(dz), other=True)


class Ring(Gather):
    def both(self, k):
        return (k, -k) if 0 < k < 4 else (self.flip * k,)

    def start(self):
        self.start_x()
        for dz in (1, -1):
            self.send(("far", 1), self.one(0, 0), dz=dz)
        self.cross_start(0, (0,))

    def near(self):
        self.got("near")
        for m in ORDER:
            for dz in (1, -1):
                self.send(("ring", 1, m), self.blk(0, m), dz=dz)
        for m in ORDER:
            self.send("early", self.blk(0, m), other=True)

    def ring(self, k, m):
        self.got(("ring", k, m))
        if k < 4:
            for side in (-1, 1):
                part = None if k < 3 else (0 if side < 0 else 1)
                self.send(("ring", k + 1, m), self.blk(side * k, m, part), dz=-side)
            for side in (-1, 1):
                self.send("early" if k < 3 else ("late", m), self.blk(side * k, m), other=True)
        else:
            self.send(("late", m), self.blk(4, m), other=True)

    def far(self, k):
        self.got(("far", k))
        for dz in self.both(k):
            if k < 3 or (k == 3 and dz * self.flip > 0):
                self.send(("far", k + 1), self.one(dz, 0), dz=1 if dz < 0 else -1)
        self.cross_start(k, self.both(k))

    def cross(self, k):
        self.cross_on(k, self.both(k))

    def cross2(self, k):
        self.cross_end(k, self.both(k), "early" if k < 3 else ("late", 0))


def split(value):
    high = value.astype(BF)
    return high, (value - high.astype(F32)).astype(BF)


CODE_SCALE, CODE_SHIFT = 250.0 / math.sqrt(0.125), 125.0


def coded(value):
    t = jnp.exp2(jnp.sqrt(jnp.abs(value)) * CODE_SCALE - CODE_SHIFT)
    return jnp.where(value < 0, -t, t).astype(BF)


def decoded(code):
    t = code.astype(F32)
    root = jnp.log(jnp.abs(t)) * (1.0 / (math.log(2.0) * CODE_SCALE)) + CODE_SHIFT / CODE_SCALE
    size = root * root
    return jnp.where(t < 0, -size, size)


def dot(a, b):
    return lax.dot_general(a, b, (((1,), (0,)), ((), ())), preferred_element_type=F32)


def kernel(
    inputs, cots, factors, first, second, master,
    own_step, own_new, copy_v, fm, sm,
    xin, cin, ct, fw, mw, wide, gt, um, own_f32,
    pa, pb, ca, cb, sa, sb, rxa, rzb, ta, tb, rza, rxb, ga, gb, nn, squares, room,
    lsem, fs_sem, fr_sem, ms_sem, mr_sem, bs_sem, br_sem,
):
    z, x, c, y = (lax.axis_index(a) for a in ("z", "x", "c", "y"))
    pos = (z, x, c, y)

    barrier = pltpu.get_barrier_semaphore()
    peers = []
    for dz in range(1, NZ):
        peers.append((lax.rem(z + dz, NZ), x, c, y))
    for dx in range(1, NX):
        peers.append((z, lax.rem(x + dx, NX), c, y))
    for dy in range(1, 4):
        peers.append((z, x, c, lax.rem(y + dy, 4)))
    peers.append((z, x, 1 - c, y))
    for peer in peers:
        pl.semaphore_signal(barrier, inc=1, device_id=peer, device_id_type=MESH)
    local = []

    def load(src, dst):
        k = pltpu.make_async_copy(src, dst, lsem.at[len(local)])
        k.start()
        local.append(k)
        return k

    fl = [load(factors.at[pl.ds(0, 2), pl.ds(8 * q, 8), :], fw.at[pl.ds(0, 2), z, x, c, q]) for q in range(4)]
    fl.append(load(factors.at[2, pl.ds(pl.multiple_of(8 * y, 8), 8), :], fw.at[2, z, x, c, y]))
    ml = load(master, own_f32)
    cl = load(cots, cin)
    xl = load(inputs, xin)
    el = [load(first, fm), load(second, sm)]

    ml.wait()
    for m in range(3):
        mw[m, z, x, c] = coded(own_f32[m]).reshape(4, 8, 256)
    for k in fl:
        k.wait()
    pl.semaphore_wait(barrier, len(peers))

    def turned(m):
        ct[pl.ds(256 * m, 256), :] = cin[m].T

    def gradient(lo, hi):
        def body(zz, _):
            at = pl.ds(pl.multiple_of(zz * 256, 256), 256)
            g_hi, g_lo = split(dot(ct[...], xin[:, at]))
            for m in range(3):
                gt[m, zz, 0:256] = g_hi[256 * m:256 * (m + 1)]
                gt[m, zz, 256:512] = g_lo[256 * m:256 * (m + 1)]
            return 0
        lax.fori_loop(lo, hi, body, 0)

    f = Direct(pos, fw, fs_sem, fr_sem, room, -1, 8)
    w = Ring(pos, mw, ms_sem, mr_sem, room, 1, 8)
    r = Copies(pos, bs_sem, br_sem, room)

    def project(m):
        both = dot(
            jnp.concatenate([gt[m, zz] for zz in range(NZ)], axis=1),
            jnp.concatenate([fw[m, zz].reshape(256, 256) for zz in range(NZ)], axis=0),
        )
        part = (both[:256] + both[256:]).T
        for half in range(2):
            cols = part[:, half * 128:(half + 1) * 128]
            if m < 2:
                for xx in range(NX):
                    pa[half, m, xx] = cols[xx * 64:(xx + 1) * 64]
            else:
                for zz in range(NZ):
                    pb[half, zz] = cols[zz * 32:(zz + 1) * 32]

    zorder = (4, 3, -3, 2, -2, 1, -1)
    xorder = (2, 1, -1)

    def widen(m):
        def body(zz, _):
            at = pl.ds(pl.multiple_of(m * D + zz * 256, 256), 256)
            wide[at, :] = decoded(mw[m, zz].reshape(256, 256))
            return 0
        lax.fori_loop(0, NZ, body, 0)

    def moments(m):
        for half in range(2):
            cols = slice(half * 128, (half + 1) * 128)
            if m < 2:
                proj = jnp.concatenate([ga[half, m, xx, zz] for xx in range(NX) for zz in range(NZ)], axis=0)
            else:
                proj = jnp.concatenate([gb[half, zz, xx] for zz in range(NZ) for xx in range(NX)], axis=0)
            nf = beta_first * fm[m, :, cols] + (1.0 - beta_first) * proj
            ns = beta_second * sm[m, :, cols] + (1.0 - beta_second) * proj * proj
            fm[m, :, cols] = nf
            sm[m, :, cols] = ns
            hi, lo = split(nf / (jnp.sqrt(ns) + adam_eps))
            nn[m, 0:256, cols] = hi
            nn[m, 256:512, cols] = lo

    def update(m):
        def body(zz, acc):
            fz = fw[m, pl.ds(4 * zz, 4)].reshape(1024, 256)
            u = dot(jnp.concatenate([fz, fz], axis=1), nn[m])
            um[m, pl.ds(pl.multiple_of(zz * 1024, 1024), 1024), :] = u
            uu = jnp.sum((u * u).reshape(128, 8, 256), axis=0)
            return acc + uu[:, :128] + uu[:, 128:]
        squares[y, m] = lax.fori_loop(0, 2, body, jnp.zeros((8, 128), F32))
        for dy in (1, 2, 3):
            r.send(("ys", m), squares.at[y, m], dy=dy)

    f.start()
    cl.wait()
    for m in range(3):
        turned(m)
    xl.wait()
    gradient(0, 2)
    f.near()
    f.quarter()
    f.far(1, NEAR_Z)
    gradient(2, 4)
    f.line_end(0, (0,), "early")
    f.far(2, FAR_Z)
    gradient(4, 6)
    f.columns()
    gradient(6, 8)
    f.ring(1, NEAR_Z, "early")
    w.start()
    f.line_end(1, NEAR_Z, "early")
    f.ring(2, FAR_Z, "late")
    f.line_end(2, FAR_Z, "late")
    f.got("early")
    f.exchange()
    w.far(1)
    w.cross(0)
    w.near()
    f.got("late")
    for m in range(2):
        project(m)
        r.send(("k", m), pa.at[1 - c, m], ca.at[m], other=True)

    def reduce_a1(m):
        r.got(("k", m))
        sa[m] = pa[c, m] + ca[m]
        for i, dx in enumerate(xorder):
            r.send(("a1", m), sa.at[m, r.xof(dx)], rxa.at[m, i], dx=dx)

    f.got("last")
    reduce_a1(0)
    project(2)
    r.send(("k", 2), pb.at[1 - c], cb, other=True)
    reduce_a1(1)
    r.got(("k", 2))
    sb[...] = pb[c] + cb[...]
    for i, dz in enumerate(zorder):
        r.send("b1", sb.at[r.zof(dz)], rzb.at[i], dz=dz)
    w.far(2)
    w.cross(1)
    w.cross2(0)
    for m in range(2):
        r.got(("a1", m))
        tot = sa[m, x]
        for i in range(3):
            tot = tot + rxa[m, i]
        for zz in range(NZ):
            ta[m, zz] = tot[zz * 8:(zz + 1) * 8]
        for i, dz in enumerate(zorder):
            r.send(("a2", m), ta.at[m, r.zof(dz)], rza.at[m, i], dz=dz)
    r.got("b1")
    tot = sb[z]
    for i in range(7):
        tot = tot + rzb[i]
    for xx in range(NX):
        tb[xx] = tot[xx * 8:(xx + 1) * 8]
    for i, dx in enumerate(xorder):
        r.send("b2", tb.at[r.xof(dx)], rxb.at[i], dx=dx)
    for m in ORDER:
        w.ring(1, m)
    w.far(3)
    w.cross(2)
    w.cross2(1)
    for m in range(2):
        r.got(("a2", m))
        tot = ta[m, z]
        for i in range(7):
            tot = tot + rza[m, i]
        ga[c, m, x, z] = tot
        for dz in zorder:
            r.send(("a3", m), ga.at[c, m, x, z], dz=dz)
    r.got("b2")
    tot = tb[x]
    for i in range(3):
        tot = tot + rxb[i]
    gb[c, z, x] = tot
    for dx in xorder:
        r.send("b3", gb.at[c, z, x], dx=dx)
    for m in ORDER:
        w.ring(2, m)
    w.far(4)
    w.cross(3)
    w.cross2(2)
    r.got("b3")
    for dz in zorder:
        r.send("b4", gb.at[c, z], dz=dz)
    for m in range(2):
        r.got(("a3", m))
        for dx in xorder:
            r.send(("a4", m), ga.at[c, m, x], dx=dx)
        r.send(("ka", m), ga.at[c, m, x], other=True)
    for k in el:
        k.wait()
    for m in ORDER:
        w.ring(3, m)
    w.cross(4)
    w.cross2(3)
    for m in range(2):
        r.got(("a4", m))
        for dx in xorder:
            r.send(("ka", m), ga.at[c, m, r.xof(-dx)], other=True)
    r.got("b4")
    r.send("kb", gb.at[c], other=True)
    w.cross2(4)
    for m in ORDER:
        w.ring(4, m)
    for m in range(2):
        r.got(("ka", m))
        moments(m)
        update(m)
    r.got("kb")
    moments(2)
    update(2)
    w.got("early")
    for m in ORDER:
        w.got(("late", m))
        widen(m)

    rows = pl.multiple_of(z * 256 + x * 64 + c * 32, 32)
    for m in ORDER:
        r.got(("ys", m))
        tot = squares[0, m]
        for j in range(1, 4):
            tot = tot + squares[j, m]
        inv = 1.0 / jnp.sqrt(jnp.sum(tot, keepdims=True) / (D * MW) + norm_eps)
        step = um[m, pl.ds(rows, 32), :] * inv
        own_step[m] = step
        own_new[m] = own_f32[m] - learning_rate * step

        def body(zz, _):
            at = pl.ds(pl.multiple_of(zz * 256, 256), 256)
            copy_v[m, at, :] = (wide[pl.ds(pl.multiple_of(m * D + zz * 256, 256), 256), :] - learning_rate * (um[m, at, :] * inv)).astype(BF)
            return 0
        lax.fori_loop(0, NZ, body, 0)
    f.drain()
    w.drain()
    r.drain()


def write_out(*refs):
    sem = refs[-1]
    copies = []
    for i in (2, 3, 4, 0, 1):
        for m in range(3):
            copies.append(pltpu.make_async_copy(refs[i].at[m], refs[5 + i].at[m], sem.at[len(copies)]))
    for k in copies:
        k.start()
    for k in copies:
        k.wait()


def local(inputs, cotangents, factors, first_moment, second_moment, master):
    cots = jnp.transpose(cotangents, (1, 0, 2))
    hbm = pl.BlockSpec(memory_space=pltpu.HBM)
    V = pltpu.VMEM
    dma = pltpu.SemaphoreType.DMA
    results = pl.pallas_call(
        kernel,
        out_shape=(
            V((3, 32, 256), F32), V((3, 32, 256), F32), V((3, D, 256), BF), V((3, 256, 256), F32), V((3, 256, 256), F32),
        ),
        in_specs=[hbm] * 6,
        out_specs=(pl.BlockSpec(memory_space=pltpu.VMEM),) * 5,
        scratch_shapes=[
            V((1024, 2048), BF), V((3, 1024, 256), BF), V((768, 1024), BF),
            V((3, NZ, NX, 2, 4, 8, 256), BF), V((3, NZ, NX, 2, 4, 8, 256), BF), V((3 * D, 256), F32),
            V((3, NZ, 512, 256), BF), V((3, D, 256), F32), V((3, 32, 256), F32),
            V((2, 2, NX, 64, 128), F32), V((2, NZ, 32, 128), F32),
            V((2, NX, 64, 128), F32), V((NZ, 32, 128), F32),
            V((2, NX, 64, 128), F32), V((NZ, 32, 128), F32),
            V((2, 3, 64, 128), F32), V((7, 32, 128), F32),
            V((2, NZ, 8, 128), F32), V((NX, 8, 128), F32),
            V((2, 7, 8, 128), F32), V((3, 8, 128), F32),
            V((2, 2, NX, NZ, 8, 128), F32), V((2, NZ, NX, 8, 128), F32),
            V((3, 512, 256), BF), V((4, 3, 8, 128), F32), V((1024, 8, 128), F32),
            dma((16,)),
            dma((1,)), dma((GROUPS,)), dma((1,)), dma((GROUPS,)),
            dma((1,)), dma((GROUPS,)),
        ],
        compiler_params=pltpu.CompilerParams(collective_id=0, has_side_effects=True, vmem_limit_bytes=58 * 1024 * 1024),
        name="update",
    )(inputs, cots, factors, first_moment, second_moment, master)
    return pl.pallas_call(
        write_out,
        out_shape=tuple(jax.ShapeDtypeStruct(r.shape, r.dtype) for r in results),
        in_specs=[pl.BlockSpec(memory_space=pl.ANY)] * 5,
        out_specs=(hbm,) * 5,
        scratch_shapes=[dma((15,))],
        compiler_params=pltpu.CompilerParams(vmem_limit_bytes=1024 * 1024),
        name="write_out",
    )(*results)


def solution(mesh):
    torus = Mesh(mesh.devices.reshape(NZ, NX, 2, mesh.shape["tp"]), ("z", "x", "c", "y"))
    fs = ("z", "x", "c")
    return jax.shard_map(
        local,
        mesh=torus,
        in_specs=(
            P(fs, None),
            P(fs, None, "y"),
            P(None, fs, None),
            P(None, None, "y"),
            P(None, None, "y"),
            P(None, fs, "y"),
        ),
        out_specs=(
            P(None, fs, "y"),
            P(None, fs, "y"),
            P(None, None, "y"),
            P(None, None, "y"),
            P(None, None, "y"),
        ),
        check_vma=False,
    )
```
